32 devices in a mesh: grp: 2 (over y), dp: 2 (over x), kv: 4 (over z), tp: 2 (over core).
Axes of the slice: x: 2, y: 2, z: 4, core: 2. Of those that a mesh axis runs over, the one named last changes fastest.
Arguments:
- inputs: bfloat16 [32, 4096], P(('grp', 'dp'), 'kv'), parts along dimension 0, may hold values from -6 to 6
- gain_in: float32 [4096], P('kv'), may hold values from 0.1 to 1.9
- w_gate: bfloat16 [4096, 2048], P('kv', 'tp'), may hold values from -0.09375 to 0.09375
- w_input: bfloat16 [4096, 2048], P('kv', 'tp'), may hold values from -0.09375 to 0.09375
- w_bproj: bfloat16 [4096, 1024], P('kv', 'tp'), may hold values from -0.09375 to 0.09375
- w_cproj: bfloat16 [4096, 1024], P('kv', 'tp'), may hold values from -0.09375 to 0.09375
- w_step: bfloat16 [4096, 32], P('kv', 'tp'), may hold values from -0.09375 to 0.09375
- conv_input: float32 [4, 2048], P(None, 'tp'), may hold values from -3 to 3
- conv_bproj: float32 [4, 1024], P(None, 'tp'), may hold values from -3 to 3
- conv_cproj: float32 [4, 1024], P(None, 'tp'), may hold values from -3 to 3
- tail_input: bfloat16 [32, 3, 2048], P(('grp', 'dp', 'kv'), None, 'tp'), parts along dimension 0, may hold values from -6 to 6
- tail_bproj: bfloat16 [32, 3, 1024], P(('grp', 'dp', 'kv'), None, 'tp'), parts along dimension 0, may hold values from -6 to 6
- tail_cproj: bfloat16 [32, 3, 1024], P(('grp', 'dp', 'kv'), None, 'tp'), parts along dimension 0, may hold values from -6 to 6
- step_bias: float32 [32], P('tp'), may hold values from -3 to 0
- decay_log: float32 [32], P('tp'), may hold values from -2 to 2
- block_input: bfloat16 [32, 128, 2048], P(('grp', 'dp', 'kv'), None, 'tp'), parts along dimension 0, may hold values from -6 to 6
- block_bproj: bfloat16 [32, 128, 1024], P(('grp', 'dp', 'kv'), None, 'tp'), parts along dimension 0, may hold values from -0.59765625 to 0.59765625
- block_step: float32 [32, 128, 32], P(('grp', 'dp', 'kv'), None, 'tp'), parts along dimension 0, may hold values from 0.005 to 0.2
- lengths: int32 [32], P(('grp', 'dp', 'kv')), parts along dimension 0, may hold values from 1 to 127, 512 in all
- state: float32 [32, 32, 64, 128], P(('grp', 'dp', 'kv'), 'tp'), parts along dimension 0, may hold values from -0.6 to 0.6
- gain_mix: float32 [2048], P('tp'), may hold values from 0.1 to 1.9
- w_out: bfloat16 [2048, 4096], P('tp', 'kv'), may hold values from -0.125 to 0.125
- gain_mlp: float32 [4096], P(('kv', 'tp')), may hold values from 0.1 to 1.9
- w_up: bfloat16 [4096, 16384], P(('kv', 'tp'), 'dp'), may hold values from -0.09375 to 0.09375
- w_down: bfloat16 [16384, 4096], P('dp', ('kv', 'tp')), may hold values from -0.046875 to 0.046875
Outputs:
- layer_out: bfloat16 [32, 4096], P(('grp', 'dp'), ('kv', 'tp')), parts along dimension 0
The draws below stay inside these ranges and needn't reach their ends.
There are 2 independent parts, one for each index of `grp`. The reference program is written for one: setup_inputs(seed, part) draws one part's arguments, and reference() takes and returns one part's arrays. A program takes and returns all parts, laid end to end along the dimension named above; an argument that names none is the same for every part. Nothing has to cross between parts.
Inputs may be any that keep to these rules, and one draw needn't show every extreme that they name: `lengths`: the number of live positions before the new token in each sequence's current block; the largest equals 127 in every draw.
All inputs are finite; a program needn't handle non-finite values.
Results may differ from the reference program's by a relative error of at most 0.012.
Values may be sent and summed in bfloat16 or wider, within the bound.
A program may use at most 64 MiB of HBM per device.

```python
import math
import jax
import jax.numpy as jnp
import numpy as np
from jax import lax

D = 4096
SSM_HEADS = 32
HEAD_DIM = 64
GROUPS = 8
D_STATE = 128
FF = 16384
TAPS = 4
BLK = 128
SSM_WIDTH = 2048
SEQS = 16


def steps_of(stream_key, dims, cuts, smallest, high):
    loudness, own = 1.0, jax.random.fold_in(stream_key, 6)
    for dim, parts in cuts:
        steps = jnp.exp(jax.random.uniform(jax.random.fold_in(own, dim), (parts,), jnp.float32, smallest / len(cuts), high / len(cuts)))
        loudness = loudness * jnp.repeat(steps, dims[dim] // parts).reshape([-1 if axis == dim else 1 for axis in range(len(dims))])
    return loudness


def split_up(number_of, total, bound, lean):
    loads = [(1 << 20) // math.isqrt(rank ** lean) + 1 for rank in range(2, number_of + 1)]
    surplus, given = total - bound - (number_of - 1), [1] * (number_of - 1)
    while surplus > 0:
        free = [i for i in range(number_of - 1) if given[i] < bound]
        mass, left = sum([loads[i] for i in free]), surplus
        for i in free:
            more = min(bound - given[i], max(1, left * loads[i] // mass), surplus)
            given[i] = given[i] + more
            surplus = surplus - more
    return np.array([bound] + given)


def uneven_parts(key, count, total, limit, slope):
    if count == 2:
        one = jax.random.randint(key, (), max(1, total - limit), min(limit, total - 1) + 1)
        return jnp.stack([one, total - one])
    sizes = jnp.asarray(split_up(count, total, limit, slope), jnp.int32)
    twos = (count - 1) // 2
    giver, taker = sizes[1:1 + 2 * twos:2], sizes[2:2 + 2 * twos:2]
    room = jnp.minimum(giver - 1, limit - taker)
    shifted = jax.random.randint(jax.random.fold_in(key, 1), (twos,), 0, 1 << 20) % (room + 1)
    sizes = sizes.at[1:1 + 2 * twos:2].set(giver - shifted).at[2:2 + 2 * twos:2].set(taker + shifted)
    return sizes[jax.random.permutation(jax.random.fold_in(key, 2), count)]


def centred(rng, extent, scale, limit, split=(), held_as=jnp.bfloat16):
    factor_of = steps_of(rng, extent, split, -0.22, 0.18) if split else 1.0
    array = jax.random.normal(rng, extent, jnp.float32) * scale * factor_of
    return jnp.minimum(jnp.maximum(array, -limit), limit).astype(held_as)


def setup_inputs(seed: int = 0, part: int = 0) -> dict:
    seeds = jax.random.split(jax.random.key(seed), 26)
    part_keys = jax.random.split(jax.random.fold_in(seeds[25], part), 26)
    inputs = centred(part_keys[0], (SEQS, D), 1.0, 6.0, ((0, 2), (1, 4)))
    gain_in = jnp.clip(1.0 + 0.18 * jax.random.normal(seeds[1], (D,), jnp.float32), 0.1, 1.9)
    w_gate = centred(seeds[2], (D, SSM_WIDTH), D ** -0.5, 0.09375, ((0, 4), (1, 2)))
    w_input = centred(seeds[3], (D, SSM_WIDTH), D ** -0.5, 0.09375, ((0, 4), (1, 2)))
    w_bproj = centred(seeds[4], (D, GROUPS * D_STATE), D ** -0.5, 0.09375, ((0, 4), (1, 2)))
    w_cproj = centred(seeds[5], (D, GROUPS * D_STATE), D ** -0.5, 0.09375, ((0, 4), (1, 2)))
    w_step = centred(seeds[6], (D, SSM_HEADS), D ** -0.5, 0.09375, ((0, 4), (1, 2)))
    conv_input = centred(seeds[7], (TAPS, SSM_WIDTH), TAPS ** -0.5, 3.0, ((1, 2),), jnp.float32)
    conv_bproj = centred(seeds[8], (TAPS, GROUPS * D_STATE), TAPS ** -0.5, 3.0, ((1, 2),), jnp.float32)
    conv_cproj = centred(seeds[9], (TAPS, GROUPS * D_STATE), TAPS ** -0.5, 3.0, ((1, 2),), jnp.float32)
    tail_input = centred(part_keys[10], (SEQS, TAPS - 1, SSM_WIDTH), 1.0, 6.0, ((0, 8), (2, 2)))
    tail_bproj = centred(part_keys[11], (SEQS, TAPS - 1, GROUPS * D_STATE), 1.0, 6.0, ((0, 8), (2, 2)))
    tail_cproj = centred(part_keys[12], (SEQS, TAPS - 1, GROUPS * D_STATE), 1.0, 6.0, ((0, 8), (2, 2)))
    step_bias = jnp.clip(-3.0 + 3.0 * jax.random.uniform(seeds[13], (SSM_HEADS,), jnp.float32) ** steps_of(seeds[13], (SSM_HEADS,), ((0, 2),), -0.2, 0.2), -3.0, 0.0)
    decay_log = jnp.clip(jax.random.uniform(seeds[14], (SSM_HEADS,), jnp.float32, -2.0, 2.0) * steps_of(seeds[14], (SSM_HEADS,), ((0, 2),), -0.4, 0.0), -2.0, 2.0)
    block_input = centred(part_keys[15], (SEQS, BLK, SSM_WIDTH), 1.0, 6.0, ((0, 8), (2, 2)))
    block_bproj = centred(part_keys[16], (SEQS, BLK, GROUPS * D_STATE), 0.1, 0.59765625, ((0, 8), (2, 2)))
    block_step = jnp.clip(jnp.exp(math.log(0.2) - 3.6888795 * jax.random.uniform(part_keys[17], (SEQS, BLK, SSM_HEADS), jnp.float32) ** steps_of(part_keys[17], (SEQS, BLK, SSM_HEADS), ((0, 8), (2, 2)), -0.2, 0.2)), 0.005, 0.2)
    lengths = uneven_parts(part_keys[18], SEQS, SEQS * BLK // 4, BLK - 1, 2).astype(jnp.int32)
    state = centred(part_keys[19], (SEQS, SSM_HEADS, HEAD_DIM, D_STATE), 0.1, 0.6, ((0, 8), (1, 2)), jnp.float32)
    gain_mix = jnp.clip(1.0 + 0.18 * jax.random.normal(seeds[20], (SSM_WIDTH,), jnp.float32), 0.1, 1.9)
    w_out = centred(seeds[21], (SSM_WIDTH, D), SSM_WIDTH ** -0.5, 0.125, ((0, 2), (1, 4)))
    gain_mlp = jnp.clip(1.0 + 0.18 * jax.random.normal(seeds[22], (D,), jnp.float32), 0.1, 1.9)
    w_up = centred(seeds[23], (D, FF), D ** -0.5, 0.09375, ((0, 8), (1, 2)))
    w_down = centred(seeds[24], (FF, D), FF ** -0.5, 0.046875, ((0, 2), (1, 8)))
    return {"inputs": inputs, "gain_in": gain_in, "w_gate": w_gate, "w_input": w_input, "w_bproj": w_bproj, "w_cproj": w_cproj, "w_step": w_step, "conv_input": conv_input, "conv_bproj": conv_bproj, "conv_cproj": conv_cproj, "tail_input": tail_input, "tail_bproj": tail_bproj, "tail_cproj": tail_cproj, "step_bias": step_bias, "decay_log": decay_log, "block_input": block_input, "block_bproj": block_bproj, "block_step": block_step, "lengths": lengths, "state": state, "gain_mix": gain_mix, "w_out": w_out, "gain_mlp": gain_mlp, "w_up": w_up, "w_down": w_down}


EPS = 1e-06

def convolve(history, weights, newest):
    summed = weights[TAPS - 1].astype(jnp.float32) * newest
    for offset in range(TAPS - 1):
        summed = summed + weights[offset].astype(jnp.float32) * history[:, offset].astype(jnp.float32)
    return jax.nn.silu(summed)

def reference(inputs, gain_in, w_gate, w_input, w_bproj, w_cproj, w_step, conv_input, conv_bproj, conv_cproj, tail_input, tail_bproj, tail_cproj, step_bias, decay_log, block_input, block_bproj, block_step, lengths, state, gain_mix, w_out, gain_mlp, w_up, w_down):
    stream = inputs.astype(jnp.float32)
    inverse = lax.rsqrt(lax.optimization_barrier(jnp.mean(stream * stream, axis=1, keepdims=True)) + EPS)
    scaled = (stream * gain_in.astype(jnp.float32)).astype(jnp.bfloat16)
    gate_pre = jnp.dot(scaled, w_gate, preferred_element_type=jnp.float32) * inverse
    value_pre = jnp.dot(scaled, w_input, preferred_element_type=jnp.float32) * inverse
    b_pre = jnp.dot(scaled, w_bproj, preferred_element_type=jnp.float32) * inverse
    c_pre = jnp.dot(scaled, w_cproj, preferred_element_type=jnp.float32) * inverse
    step_pre = jnp.dot(scaled, w_step, preferred_element_type=jnp.float32) * inverse
    current = convolve(tail_input, conv_input, value_pre)
    b_now = convolve(tail_bproj, conv_bproj, b_pre)
    c_now = convolve(tail_cproj, conv_cproj, c_pre)
    step_size = jax.nn.softplus(step_pre + step_bias.astype(jnp.float32))
    decay_rate = -jnp.exp(decay_log.astype(jnp.float32))
    positions = jnp.arange(BLK, dtype=jnp.int32)
    live_rows = (positions[None, :] < lengths[:, None].astype(jnp.int32)).astype(jnp.float32)
    block_steps = block_step.astype(jnp.float32)
    masked = block_steps * live_rows[:, :, None]
    later_steps = lax.optimization_barrier(jnp.sum(masked, axis=1, keepdims=True)) - jnp.cumsum(masked, axis=1)
    decays = jnp.exp(decay_rate * (step_size[:, None, :] + later_steps)) * live_rows[:, :, None]
    per_group = SSM_HEADS // GROUPS
    c_query = lax.optimization_barrier(c_now.astype(jnp.bfloat16)).astype(jnp.float32).reshape(SEQS, GROUPS, D_STATE)
    keys = block_bproj.astype(jnp.float32).reshape(SEQS, BLK, GROUPS, D_STATE)
    scores = jnp.repeat(jnp.einsum('bsgn,bgn->bsg', keys, c_query), per_group, axis=2)
    weights = lax.optimization_barrier((decays * scores * block_steps).astype(jnp.bfloat16)).astype(jnp.float32)
    values = block_input.astype(jnp.float32).reshape(SEQS, BLK, SSM_HEADS, HEAD_DIM)
    inner_sum = jnp.einsum('bsh,bshp->bhp', weights, values)
    c_full = c_now.reshape(SEQS, GROUPS, D_STATE)
    b_full = b_now.reshape(SEQS, GROUPS, D_STATE)
    own_score = jnp.repeat(lax.optimization_barrier(jnp.sum(c_full * b_full, axis=2)), per_group, axis=1)
    own_term = (step_size * own_score)[:, :, None] * current.reshape(SEQS, SSM_HEADS, HEAD_DIM)
    carried = jnp.exp(decay_rate * (step_size + lax.optimization_barrier(jnp.sum(masked, axis=1))))
    c_heads = jnp.repeat(c_full, per_group, axis=1)
    readout = jnp.einsum('bhpn,bhn->bhp', state.astype(jnp.float32), c_heads, precision=lax.Precision.HIGHEST)
    mixed = (inner_sum + own_term + carried[:, :, None] * readout).reshape(SEQS, SSM_WIDTH) * jax.nn.silu(gate_pre)
    inverse_mix = lax.rsqrt(lax.optimization_barrier(jnp.mean(mixed * mixed, axis=1, keepdims=True)) + EPS)
    normed = (mixed * inverse_mix * gain_mix.astype(jnp.float32)).astype(jnp.bfloat16)
    hidden = (stream + jnp.dot(normed, w_out, preferred_element_type=jnp.float32)).astype(jnp.bfloat16)
    hidden_f = hidden.astype(jnp.float32)
    inverse_mlp = lax.rsqrt(lax.optimization_barrier(jnp.mean(hidden_f * hidden_f, axis=1, keepdims=True)) + EPS)
    lifted = (hidden_f * gain_mlp.astype(jnp.float32)).astype(jnp.bfloat16)
    raised = jnp.dot(lifted, w_up, preferred_element_type=jnp.float32) * inverse_mlp
    hidden_units = jnp.square(jax.nn.relu(raised)).astype(jnp.bfloat16)
    return (hidden_f + jnp.dot(hidden_units, w_down, preferred_element_type=jnp.float32)).astype(jnp.bfloat16)
```

```python
import functools

import jax
import jax.numpy as jnp
from jax import lax
from jax.experimental import pallas as pl
from jax.experimental.pallas import tpu as pltpu
from jax.sharding import PartitionSpec as P

D = 4096
HEAD_DIM = 64
D_STATE = 128
TAPS = 4
SSM_WIDTH = 2048


EPS = 1e-06


def convolve(history, weights, newest):
    summed = weights[TAPS - 1] * newest
    for offset in range(TAPS - 1):
        summed = summed + weights[offset] * history[:, offset].astype(jnp.float32)
    return jax.nn.silu(summed)


def per_device(
    inputs,
    gain_in,
    w_gate,
    w_input,
    w_bproj,
    w_cproj,
    w_step,
    conv_input,
    conv_bproj,
    conv_cproj,
    tail_input,
    tail_bproj,
    tail_cproj,
    step_bias,
    decay_log,
    block_input,
    block_bproj,
    block_step,
    lengths,
    state,
    gain_mix,
    w_out,
    gain_mlp,
    w_up,
    w_down,
):
    stream = inputs.astype(jnp.float32)
    squares = jnp.sum(stream * stream, axis=1)
    scaled = (stream * gain_in).astype(jnp.bfloat16)
    matrices = (w_gate, w_input, w_bproj, w_cproj, w_step)
    pieces = [jnp.dot(scaled, weight, preferred_element_type=jnp.float32) for weight in matrices]
    projected, totals = (
        lax.psum_scatter(jnp.concatenate(pieces, axis=1), "kv", scatter_dimension=0, tiled=True),
        lax.psum_scatter(squares, "kv", scatter_dimension=0, tiled=True),
    )
    inverse = lax.rsqrt(totals / D + EPS)[:, None]
    bounds = [0]
    for weight in matrices:
        bounds.append(bounds[-1] + weight.shape[1])
    gate_pre, value_pre, b_pre, c_pre, step_pre = [
        projected[:, bounds[member] : bounds[member + 1]] * inverse for member in range(5)
    ]
    seq_count = lengths.shape[0]
    head_count = step_bias.shape[0]
    group_count = w_bproj.shape[1] // D_STATE
    block_len = block_step.shape[1]
    per_group = head_count // group_count
    current = convolve(tail_input, conv_input, value_pre)
    b_now = convolve(tail_bproj, conv_bproj, b_pre)
    c_now = convolve(tail_cproj, conv_cproj, c_pre)
    step_size = jax.nn.softplus(step_pre + step_bias)
    decay_rate = -jnp.exp(decay_log)
    positions = lax.broadcasted_iota(jnp.int32, (1, block_len), 1)
    live_rows = (positions < lengths[:, None]).astype(jnp.float32)
    masked = block_step * live_rows[:, :, None]
    later_steps = jnp.sum(masked, axis=1, keepdims=True) - jnp.cumsum(masked, axis=1)
    decays = jnp.exp(decay_rate * (step_size[:, None, :] + later_steps)) * live_rows[:, :, None]
    c_query = c_now.astype(jnp.bfloat16).reshape(seq_count, group_count, D_STATE)
    keys = block_bproj.reshape(seq_count, block_len, group_count, D_STATE)
    scores = jnp.einsum("bsgn,bgn->bsg", keys, c_query, preferred_element_type=jnp.float32)
    scores = jnp.repeat(scores, per_group, axis=2)
    weights = (decays * scores * block_step).astype(jnp.bfloat16)
    values = block_input.reshape(seq_count, block_len, head_count, HEAD_DIM)
    inner_sum = jnp.einsum("bsh,bshp->bhp", weights, values, preferred_element_type=jnp.float32)
    c_full = c_now.reshape(seq_count, group_count, D_STATE)
    b_full = b_now.reshape(seq_count, group_count, D_STATE)
    own_score = jnp.repeat(jnp.sum(c_full * b_full, axis=2), per_group, axis=1)
    own_term = (step_size * own_score)[:, :, None] * current.reshape(
        seq_count, head_count, HEAD_DIM
    )
    carried = jnp.exp(decay_rate * (step_size + jnp.sum(masked, axis=1)))
    c_heads = jnp.repeat(c_full, per_group, axis=1)
    readout = jnp.einsum("bhpn,bhn->bhp", state, c_heads, precision=lax.Precision.HIGHEST)
    mixed = (inner_sum + own_term + carried[:, :, None] * readout).reshape(
        seq_count, -1
    ) * jax.nn.silu(gate_pre)
    local_sq = jnp.sum(mixed * mixed, axis=1)
    total_sq = lax.psum(local_sq, "tp")
    normed = (mixed * lax.rsqrt(total_sq / SSM_WIDTH + EPS)[:, None] * gain_mix).astype(
        jnp.bfloat16
    )
    products = jnp.dot(
        lax.all_gather(normed, "kv", axis=0, tiled=True), w_out, preferred_element_type=jnp.float32
    )
    mixed_in = lax.psum_scatter(products, "tp", scatter_dimension=1, tiled=True)
    column_count = mixed_in.shape[1]
    residual = lax.dynamic_slice_in_dim(
        stream, lax.axis_index("tp") * column_count, column_count, 1
    )
    hidden = (residual + mixed_in).astype(jnp.bfloat16)
    lifted = (hidden.astype(jnp.float32) * gain_mlp).astype(jnp.bfloat16)
    all_lifted, all_hidden = (
        lax.all_gather(lifted, "dp", axis=0, tiled=True),
        lax.all_gather(hidden, "dp", axis=0, tiled=True),
    )
    whole_rows = all_hidden.astype(jnp.float32)
    row_sq = jnp.sum(whole_rows * whole_rows, axis=1)
    partial_value = jnp.dot(all_lifted, w_up, preferred_element_type=jnp.float32)
    sq_sum = lax.psum(row_sq, ("kv", "tp"))
    shares = lax.psum_scatter(partial_value, ("kv", "tp"), scatter_dimension=1, tiled=True)
    unit_share = jnp.square(jax.nn.relu(shares * lax.rsqrt(sq_sum / D + EPS)[:, None])).astype(
        jnp.bfloat16
    )
    hidden_units = lax.all_gather(unit_share, ("kv", "tp"), axis=1, tiled=True)
    lowered = lax.psum_scatter(
        jnp.dot(hidden_units, w_down, preferred_element_type=jnp.float32),
        "dp",
        scatter_dimension=0,
        tiled=True,
    )
    return (hidden.astype(jnp.float32) + lowered).astype(jnp.bfloat16)


MESH = pl.DeviceIdType.MESH
LANES = 128
F32 = jnp.float32
BF16 = jnp.bfloat16

(
    INPUTS,
    GAIN_IN,
    W_GATE,
    W_INPUT,
    W_BPROJ,
    W_CPROJ,
    W_STEP,
    CONV_INPUT,
    CONV_BPROJ,
    CONV_CPROJ,
    TAIL_INPUT,
    TAIL_BPROJ,
    TAIL_CPROJ,
    STEP_BIAS,
    DECAY_LOG,
    BLOCK_INPUT,
    BLOCK_BPROJ,
    BLOCK_STEP,
    LENGTHS,
    STATE,
    GAIN_MIX,
    W_OUT,
    GAIN_MLP,
    W_UP,
    W_DOWN,
) = NAMES = range(25)
EARLY = (
    INPUTS, GAIN_IN, W_STEP, W_GATE, W_INPUT, W_BPROJ, W_CPROJ,
)
MIDDLE = (
    CONV_INPUT, CONV_BPROJ, CONV_CPROJ, TAIL_INPUT, TAIL_BPROJ, TAIL_CPROJ,
    STEP_BIAS, DECAY_LOG, BLOCK_STEP, BLOCK_BPROJ, BLOCK_INPUT, STATE,
    GAIN_MIX, W_OUT, GAIN_MLP,
)
LATE = (W_UP, W_DOWN)
COPIED = EARLY + MIDDLE + LATE


def send(source, target, send_sem, recv_sem, device):
    copy = pltpu.make_async_remote_copy(
        src_ref=source,
        dst_ref=target,
        send_sem=send_sem,
        recv_sem=recv_sem,
        device_id=device,
        device_id_type=MESH,
    )
    copy.start()
    return copy


def taps(history, weights, newest):
    past = history.astype(F32)
    summed = weights[TAPS - 1 :] * newest
    for offset in range(TAPS - 1):
        summed = summed + weights[offset : offset + 1] * past[offset : offset + 1]
    return summed * lax.logistic(summed)


def fused(sizes, *refs):
    kv, tp, dp = sizes
    hbm = dict(zip(NAMES, refs[: len(NAMES)]))
    out_ref = refs[len(NAMES)]
    rest = list(refs[len(NAMES) + 1 :])
    vm = dict(zip(COPIED, rest[: len(COPIED)]))
    (
        a_send, a_recv, g_buf, p_send, p_recv, h_buf, q_buf, u_send, u_recv, r_send, r_recv, own_sum,
        units, l_send, l_recv,
        local_sem, a_ss, a_rs, g_ss, g_rs, p_ss, p_rs, h_ss, h_rs, q_ss, q_rs, u_ss, u_rs,
        r_ss, r_rs, n_ss, n_rs, f_ss, f_rs, l_ss, l_rs,
    ) = rest[len(COPIED) :]
    me_kv, me_tp, me_dp = lax.axis_index("kv"), lax.axis_index("tp"), lax.axis_index("dp")
    me_unit = me_kv * tp + me_tp

    def kv_peer(j):
        return lax.rem(me_kv + j, kv)

    def tp_peer(q):
        return lax.rem(me_tp + q, tp)

    def dp_peer(d):
        return lax.rem(me_dp + d, dp)

    pairs = [(j, q) for j in range(kv) for q in range(tp) if j or q]
    far_first = sorted(range(kv), key=lambda j: -min(j, kv - j))
    near_first = [j for j in reversed(far_first) if j]

    barrier = pltpu.get_barrier_semaphore()
    for j, q in pairs:
        pl.semaphore_signal(
            barrier, inc=1, device_id={"kv": kv_peer(j), "tp": tp_peer(q)}, device_id_type=MESH
        )
    for d in range(1, dp):
        pl.semaphore_signal(barrier, inc=1, device_id={"dp": dp_peer(d)}, device_id_type=MESH)

    local = {
        name: pltpu.make_async_copy(hbm[name], vm[name], local_sem.at[index])
        for index, name in enumerate(COPIED)
    }
    for name in EARLY + MIDDLE:
        local[name].start()
    pending = []

    local[INPUTS].wait()
    local[GAIN_IN].wait()
    stream = vm[INPUTS][...].astype(F32)
    rows = stream.shape[0]
    seqs = rows // kv
    scaled = (stream * vm[GAIN_IN][...]).astype(BF16)
    squares = jnp.sum(stream * stream, axis=1, keepdims=True)
    offsets = {}
    at = 0
    for name in (W_GATE, W_INPUT, W_BPROJ, W_CPROJ, W_STEP):
        width = vm[name].shape[1]
        offsets[name] = at
        local[name].wait()
        piece = jnp.dot(scaled, vm[name][...], preferred_element_type=F32)
        for k in range(kv):
            a_send[k, :, at : at + width] = piece[k * seqs : (k + 1) * seqs]
        at += -(-width // LANES) * LANES
    wide_squares = jnp.broadcast_to(squares, (rows, LANES))
    for k in range(kv):
        a_send[k, :, at : at + LANES] = wide_squares[k * seqs : (k + 1) * seqs]
    for name in LATE:
        local[name].start()
    pl.semaphore_wait(barrier, len(pairs) + dp - 1)
    copies = [
        send(a_send.at[kv_peer(j)], a_recv.at[j - 1], a_ss.at[j - 1], a_rs.at[j - 1], {"kv": kv_peer(j)})
        for j in far_first
        if j
    ]

    for name in MIDDLE[:-3]:
        local[name].wait()
    heads = vm[STEP_BIAS].shape[1]
    groups = vm[W_BPROJ].shape[1] // D_STATE
    per_group = heads // groups
    channels = heads * HEAD_DIM
    block = vm[BLOCK_STEP].shape[1]
    head_eye = lax.broadcasted_iota(jnp.int32, (heads, heads), 0) == lax.broadcasted_iota(
        jnp.int32, (heads, heads), 1
    )
    eye = head_eye.astype(F32)

    def column(row):
        return jnp.sum(jnp.where(head_eye, row, 0.0), axis=1, keepdims=True)

    later_than = (
        lax.broadcasted_iota(jnp.int32, (block, block), 0)
        > lax.broadcasted_iota(jnp.int32, (block, block), 1)
    ).astype(F32)
    positions = lax.broadcasted_iota(jnp.int32, (heads, block), 1)
    decay_rate = column(-jnp.exp(vm[DECAY_LOG][...]))
    prepared = []
    for b in range(seqs):
        live = positions < hbm[LENGTHS][b]
        steps = lax.dot_general(
            eye,
            vm[BLOCK_STEP][b],
            (((1,), (1,)), ((), ())),
            precision=lax.Precision.HIGHEST,
            preferred_element_type=F32,
        )
        masked = jnp.where(live, steps, 0.0)
        later = jnp.dot(
            masked, later_than, precision=lax.Precision.HIGHEST, preferred_element_type=F32
        )
        prepared.append((live, steps, later, jnp.sum(masked, axis=1, keepdims=True)))
    own_head = lax.broadcasted_iota(jnp.int32, (heads, channels), 0) == (
        lax.broadcasted_iota(jnp.int32, (heads, channels), 1) // HEAD_DIM
    )
    own_group = (lax.broadcasted_iota(jnp.int32, (heads, groups * D_STATE), 0) // per_group) == (
        lax.broadcasted_iota(jnp.int32, (heads, groups * D_STATE), 1) // D_STATE
    )

    projected = a_send[me_kv]
    for copy, j in zip(copies, [j for j in far_first if j]):
        copy.wait_recv()
        projected = projected + a_recv[j - 1]
    pending += copies
    features = vm[INPUTS].shape[1] * kv
    inverse = lax.rsqrt(projected[:, at : at + 1] / features + EPS)

    def part(name):
        start = offsets[name]
        return projected[:, start : start + vm[name].shape[1]] * inverse

    gate_pre, value_pre, b_pre, c_pre, step_pre = [
        part(name) for name in (W_GATE, W_INPUT, W_BPROJ, W_CPROJ, W_STEP)
    ]
    biased = step_pre + vm[STEP_BIAS][...]
    softened = jnp.maximum(biased, 0.0) + jnp.log1p(jnp.exp(-jnp.abs(biased)))
    mixed_rows = []
    for b in range(seqs):
        live, steps, later, total_steps = prepared[b]
        current = taps(vm[TAIL_INPUT][b], vm[CONV_INPUT][...], value_pre[b : b + 1])
        b_now = taps(vm[TAIL_BPROJ][b], vm[CONV_BPROJ][...], b_pre[b : b + 1])
        c_now = taps(vm[TAIL_CPROJ][b], vm[CONV_CPROJ][...], c_pre[b : b + 1])
        step_size = column(softened[b : b + 1])
        c_spread = jnp.where(own_group, c_now, 0.0)
        scores = lax.dot_general(
            c_spread.astype(BF16),
            vm[BLOCK_BPROJ][b],
            (((1,), (1,)), ((), ())),
            preferred_element_type=F32,
        )
        decays = jnp.where(live, jnp.exp(decay_rate * (step_size + later)), 0.0)
        weights = (decays * scores * steps).astype(BF16)
        inner = jnp.dot(weights, vm[BLOCK_INPUT][b], preferred_element_type=F32)
        own_score = jnp.sum(c_spread * b_now, axis=1, keepdims=True)
        carried = jnp.exp(decay_rate * (step_size + total_steps))
        c_heads = sum(
            c_spread[:, g * D_STATE : (g + 1) * D_STATE] for g in range(groups)
        )
        readout = lax.dot_general(
            c_heads,
            vm[STATE][b].reshape(channels, D_STATE),
            (((1,), (1,)), ((), ())),
            precision=lax.Precision.HIGHEST,
            preferred_element_type=F32,
        )
        terms = inner + (step_size * own_score) * current + carried * readout
        mixed_rows.append(jnp.sum(jnp.where(own_head, terms, 0.0), axis=0, keepdims=True))
    mixed = jnp.concatenate(mixed_rows, axis=0) * (gate_pre * lax.logistic(gate_pre))
    local[GAIN_MIX].wait()
    g_buf[me_kv, :, :channels] = mixed * vm[GAIN_MIX][...]
    g_buf[me_kv, :, channels:] = jnp.broadcast_to(
        jnp.sum(mixed * mixed, axis=1, keepdims=True), (seqs, LANES)
    )
    copies = [
        send(g_buf.at[me_kv], g_buf.at[me_kv], g_ss.at[j - 1], g_rs.at[j - 1], {"kv": kv_peer(j)})
        for j in far_first
        if j
    ]
    local[W_OUT].wait()
    local[GAIN_MLP].wait()
    for copy in copies:
        copy.wait_recv()
    pending += copies

    gathered = jnp.concatenate([g_buf[k] for k in range(kv)], axis=0)
    unscaled = gathered[:, :channels].astype(BF16)
    share = vm[W_OUT].shape[1] // tp
    for q in range(tp):
        p_send[q, :, :share] = jnp.dot(
            unscaled, vm[W_OUT][:, q * share : (q + 1) * share], preferred_element_type=F32
        )
        p_send[q, :, share:] = gathered[:, channels:]
    copies = [
        send(p_send.at[tp_peer(q)], p_recv.at[q - 1], p_ss.at[q - 1], p_rs.at[q - 1], {"tp": tp_peer(q)})
        for q in range(1, tp)
    ]
    residual = stream[:, :share]
    for q in range(1, tp):
        residual = jnp.where(me_tp == q, stream[:, q * share : (q + 1) * share], residual)
    summed = p_send[me_tp]
    for q, copy in enumerate(copies):
        copy.wait_recv()
        summed = summed + p_recv[q]
    pending += copies
    mixed_in = summed[:, :share] * lax.rsqrt(summed[:, share : share + 1] / (channels * tp) + EPS)
    hidden = (residual + mixed_in).astype(BF16).astype(F32)
    h_buf[me_dp] = hidden
    copies = [
        send(h_buf.at[me_dp], h_buf.at[me_dp], h_ss.at[d - 1], h_rs.at[d - 1], {"dp": dp_peer(d)})
        for d in range(1, dp)
    ]
    local[W_UP].wait()
    for copy in copies:
        copy.wait_recv()
    pending += copies

    whole_rows = jnp.concatenate([h_buf[d] for d in range(dp)], axis=0)
    lifted = (whole_rows * vm[GAIN_MLP][...]).astype(BF16)
    all_rows = rows * dp
    row_eye = lax.broadcasted_iota(jnp.int32, (all_rows, q_buf.shape[2]), 0) == (
        lax.broadcasted_iota(jnp.int32, (all_rows, q_buf.shape[2]), 1)
    )
    row_sq = jnp.sum(whole_rows * whole_rows, axis=1, keepdims=True)
    q_buf[0] = jnp.sum(jnp.where(row_eye, row_sq, 0.0), axis=0, keepdims=True)
    q_copies = [
        send(
            q_buf.at[0],
            q_buf.at[slot],
            q_ss.at[slot - 1],
            q_rs.at[slot - 1],
            {"kv": kv_peer(j), "tp": tp_peer(q)},
        )
        for slot, (j, q) in enumerate(pairs, 1)
    ]
    unit_share = vm[W_UP].shape[1] // (kv * tp)

    def raised(j, q):
        chunk = kv_peer(j) * tp + tp_peer(q)
        columns = pl.ds(pl.multiple_of(chunk * unit_share, LANES), unit_share)
        return jnp.dot(lifted, vm[W_UP][:, columns], preferred_element_type=F32)

    u_copies = {}
    for j in far_first:
        for q in range(1, tp):
            u_send[q - 1, j] = raised(j, q)
            u_copies[j, q] = send(
                u_send.at[q - 1, j],
                u_recv.at[q - 1, j],
                u_ss.at[q - 1, j],
                u_rs.at[q - 1, j],
                {"tp": tp_peer(q)},
            )
    r_copies = {}
    for j in far_first:
        total = raised(j, 0)
        for q in range(1, tp):
            u_copies[j, q].wait_recv()
            total = total + u_recv[q - 1, j]
        if j:
            r_send[j - 1] = total.astype(BF16)
            r_copies[j] = send(
                r_send.at[j - 1], r_recv.at[j - 1], r_ss.at[j - 1], r_rs.at[j - 1], {"kv": kv_peer(j)}
            )
        else:
            own_sum[...] = total
    pending += list(u_copies.values()) + list(r_copies.values()) + q_copies
    sq_row = q_buf[0]
    for slot, copy in enumerate(q_copies, 1):
        copy.wait_recv()
        sq_row = sq_row + q_buf[slot]
    sq_sum = jnp.sum(jnp.where(row_eye, sq_row, 0.0), axis=1, keepdims=True)
    inverse_mlp = lax.rsqrt(sq_sum / features + EPS)
    shares = own_sum[...]
    for j in near_first:
        r_copies[j].wait_recv()
        shares = shares + r_recv[j - 1].astype(F32)
    active = jnp.maximum(shares * inverse_mlp, 0.0)
    units[me_unit] = (active * active).astype(BF16)

    n_copies = {}
    for j in far_first:
        if j:
            n_copies[j] = send(
                units.at[me_unit], units.at[me_unit], n_ss.at[j - 1], n_rs.at[j - 1], {"kv": kv_peer(j)}
            )
    f_copies = {}

    def forward(j):
        for q in range(1, tp):
            chunk = lax.rem(me_kv + kv - j, kv) * tp + me_tp
            f_copies[j, q] = send(
                units.at[chunk], units.at[chunk], f_ss.at[q - 1, j], f_rs.at[q - 1, j], {"tp": tp_peer(q)}
            )

    def lower(j, q):
        chunk = lax.rem(me_kv + kv - j, kv) * tp + lax.rem(me_tp + tp - q, tp)
        span = pl.ds(pl.multiple_of(chunk * unit_share, LANES), unit_share)
        return jnp.dot(units[chunk], vm[W_DOWN][span, :], preferred_element_type=F32)

    forward(0)
    local[W_DOWN].wait()
    lowered = lower(0, 0)
    for q in range(1, tp):
        f_copies[0, q].wait_recv()
        lowered = lowered + lower(0, q)
    for j in near_first:
        n_copies[j].wait_recv()
        forward(j)
        lowered = lowered + lower(j, 0)
    for j in near_first:
        for q in range(1, tp):
            f_copies[j, q].wait_recv()
            lowered = lowered + lower(j, q)
    pending += list(n_copies.values()) + list(f_copies.values())

    for d in range(dp):
        l_send[d] = lowered[d * rows : (d + 1) * rows]
    copies = [
        send(l_send.at[dp_peer(d)], l_recv.at[d - 1], l_ss.at[d - 1], l_rs.at[d - 1], {"dp": dp_peer(d)})
        for d in range(1, dp)
    ]
    for copy in pending:
        copy.wait_send()
    result = h_buf[me_dp] + l_send[me_dp]
    for d, copy in enumerate(copies):
        copy.wait_recv()
        result = result + l_recv[d]
    out_ref[...] = result.astype(BF16)
    for copy in copies:
        copy.wait_send()


def fused_device(sizes, *args):
    kv, tp, dp = sizes
    named = dict(zip(NAMES, args))
    for name in (GAIN_IN, STEP_BIAS, DECAY_LOG, GAIN_MIX, GAIN_MLP):
        named[name] = named[name].reshape(1, -1)
    rows = named[INPUTS].shape[0]
    seqs = rows // kv
    pads = [
        -(-named[name].shape[1] // LANES) * LANES
        for name in (W_GATE, W_INPUT, W_BPROJ, W_CPROJ, W_STEP)
    ]
    wide = sum(pads) + LANES
    channels = named[W_GATE].shape[1]
    share = named[W_OUT].shape[1] // tp
    all_rows = rows * dp
    unit_share = named[W_UP].shape[1] // (kv * tp)
    columns = named[W_DOWN].shape[1]
    row_lanes = -(-all_rows // LANES) * LANES
    dma = pltpu.SemaphoreType.DMA
    scratch = [pltpu.VMEM(named[name].shape, named[name].dtype) for name in COPIED] + [
        pltpu.VMEM((kv, seqs, wide), F32),
        pltpu.VMEM((kv - 1, seqs, wide), F32),
        pltpu.VMEM((kv, seqs, channels + LANES), F32),
        pltpu.VMEM((tp, rows, share + LANES), F32),
        pltpu.VMEM((tp - 1, rows, share + LANES), F32),
        pltpu.VMEM((dp, rows, share), F32),
        pltpu.VMEM((kv * tp, 1, row_lanes), F32),
        pltpu.VMEM((tp - 1, kv, all_rows, unit_share), F32),
        pltpu.VMEM((tp - 1, kv, all_rows, unit_share), F32),
        pltpu.VMEM((kv - 1, all_rows, unit_share), BF16),
        pltpu.VMEM((kv - 1, all_rows, unit_share), BF16),
        pltpu.VMEM((all_rows, unit_share), F32),
        pltpu.VMEM((kv * tp, all_rows, unit_share), BF16),
        pltpu.VMEM((dp, rows, columns), F32),
        pltpu.VMEM((dp - 1, rows, columns), F32),
        dma((len(COPIED),)),
        dma((kv - 1,)), dma((kv - 1,)),
        dma((kv - 1,)), dma((kv - 1,)),
        dma((tp - 1,)), dma((tp - 1,)),
        dma((dp - 1,)), dma((dp - 1,)),
        dma((kv * tp - 1,)), dma((kv * tp - 1,)),
        dma((tp - 1, kv)), dma((tp - 1, kv)),
        dma((kv - 1,)), dma((kv - 1,)),
        dma((kv - 1,)), dma((kv - 1,)),
        dma((tp - 1, kv)), dma((tp - 1, kv)),
        dma((dp - 1,)), dma((dp - 1,)),
    ]
    spaces = [
        pl.BlockSpec(memory_space=pltpu.SMEM if name == LENGTHS else pl.ANY) for name in NAMES
    ]
    return pl.pallas_call(
        functools.partial(fused, sizes),
        out_shape=jax.ShapeDtypeStruct((rows, columns), BF16),
        in_specs=spaces,
        out_specs=pl.BlockSpec(memory_space=pltpu.VMEM),
        scratch_shapes=scratch,
        compiler_params=pltpu.CompilerParams(
            collective_id=0, has_side_effects=True, vmem_limit_bytes=60 * 1024 * 1024
        ),
    )(*[named[name] for name in NAMES])


def choose(sizes, *args):
    kv, tp, _ = sizes
    named = dict(zip(NAMES, args))
    pieces = (named[W_UP].shape[1] // (kv * tp), named[W_OUT].shape[1] // tp)
    if min(sizes) > 1 and all(piece % LANES == 0 for piece in pieces):
        return fused_device(sizes, *args)
    return per_device(*args)


def solution(mesh):
    sizes = tuple(mesh.shape[axis] for axis in ("kv", "tp", "dp"))
    return jax.shard_map(
        functools.partial(choose, sizes),
        mesh=mesh,
        in_specs=(
            P(("grp", "dp"), "kv"),
            P("kv"),
            P("kv", "tp"),
            P("kv", "tp"),
            P("kv", "tp"),
            P("kv", "tp"),
            P("kv", "tp"),
            P(None, "tp"),
            P(None, "tp"),
            P(None, "tp"),
            P(("grp", "dp", "kv"), None, "tp"),
            P(("grp", "dp", "kv"), None, "tp"),
            P(("grp", "dp", "kv"), None, "tp"),
            P("tp"),
            P("tp"),
            P(("grp", "dp", "kv"), None, "tp"),
            P(("grp", "dp", "kv"), None, "tp"),
            P(("grp", "dp", "kv"), None, "tp"),
            P(("grp", "dp", "kv")),
            P(("grp", "dp", "kv"), "tp", None, None),
            P("tp"),
            P("tp", "kv"),
            P(("kv", "tp")),
            P(("kv", "tp"), "dp"),
            P("dp", ("kv", "tp")),
        ),
        out_specs=P(("grp", "dp"), ("kv", "tp")),
        check_vma=False,
    )
```

```python
import functools

import jax
import jax.numpy as jnp
from jax import lax
from jax.experimental import pallas as pl
from jax.experimental.pallas import tpu as pltpu
from jax.sharding import PartitionSpec as P

D = 4096
HEAD_DIM = 64
D_STATE = 128
TAPS = 4
SSM_WIDTH = 2048


EPS = 1e-06


def convolve(history, weights, newest):
    summed = weights[TAPS - 1] * newest
    for offset in range(TAPS - 1):
        summed = summed + weights[offset] * history[:, offset].astype(jnp.float32)
    return jax.nn.silu(summed)


def per_device(
    inputs,
    gain_in,
    w_gate,
    w_input,
    w_bproj,
    w_cproj,
    w_step,
    conv_input,
    conv_bproj,
    conv_cproj,
    tail_input,
    tail_bproj,
    tail_cproj,
    step_bias,
    decay_log,
    block_input,
    block_bproj,
    block_step,
    lengths,
    state,
    gain_mix,
    w_out,
    gain_mlp,
    w_up,
    w_down,
):
    stream = inputs.astype(jnp.float32)
    squares = jnp.sum(stream * stream, axis=1)
    scaled = (stream * gain_in).astype(jnp.bfloat16)
    matrices = (w_gate, w_input, w_bproj, w_cproj, w_step)
    pieces = [jnp.dot(scaled, weight, preferred_element_type=jnp.float32) for weight in matrices]
    projected, totals = (
        lax.psum_scatter(jnp.concatenate(pieces, axis=1), "kv", scatter_dimension=0, tiled=True),
        lax.psum_scatter(squares, "kv", scatter_dimension=0, tiled=True),
    )
    inverse = lax.rsqrt(totals / D + EPS)[:, None]
    bounds = [0]
    for weight in matrices:
        bounds.append(bounds[-1] + weight.shape[1])
    gate_pre, value_pre, b_pre, c_pre, step_pre = [
        projected[:, bounds[member] : bounds[member + 1]] * inverse for member in range(5)
    ]
    seq_count = lengths.shape[0]
    head_count = step_bias.shape[0]
    group_count = w_bproj.shape[1] // D_STATE
    block_len = block_step.shape[1]
    per_group = head_count // group_count
    current = convolve(tail_input, conv_input, value_pre)
    b_now = convolve(tail_bproj, conv_bproj, b_pre)
    c_now = convolve(tail_cproj, conv_cproj, c_pre)
    step_size = jax.nn.softplus(step_pre + step_bias)
    decay_rate = -jnp.exp(decay_log)
    positions = lax.broadcasted_iota(jnp.int32, (1, block_len), 1)
    live_rows = (positions < lengths[:, None]).astype(jnp.float32)
    masked = block_step * live_rows[:, :, None]
    later_steps = jnp.sum(masked, axis=1, keepdims=True) - jnp.cumsum(masked, axis=1)
    decays = jnp.exp(decay_rate * (step_size[:, None, :] + later_steps)) * live_rows[:, :, None]
    c_query = c_now.astype(jnp.bfloat16).reshape(seq_count, group_count, D_STATE)
    keys = block_bproj.reshape(seq_count, block_len, group_count, D_STATE)
    scores = jnp.einsum("bsgn,bgn->bsg", keys, c_query, preferred_element_type=jnp.float32)
    scores = jnp.repeat(scores, per_group, axis=2)
    weights = (decays * scores * block_step).astype(jnp.bfloat16)
    values = block_input.reshape(seq_count, block_len, head_count, HEAD_DIM)
    inner_sum = jnp.einsum("bsh,bshp->bhp", weights, values, preferred_element_type=jnp.float32)
    c_full = c_now.reshape(seq_count, group_count, D_STATE)
    b_full = b_now.reshape(seq_count, group_count, D_STATE)
    own_score = jnp.repeat(jnp.sum(c_full * b_full, axis=2), per_group, axis=1)
    own_term = (step_size * own_score)[:, :, None] * current.reshape(
        seq_count, head_count, HEAD_DIM
    )
    carried = jnp.exp(decay_rate * (step_size + jnp.sum(masked, axis=1)))
    c_heads = jnp.repeat(c_full, per_group, axis=1)
    readout = jnp.einsum("bhpn,bhn->bhp", state, c_heads, precision=lax.Precision.HIGHEST)
    mixed = (inner_sum + own_term + carried[:, :, None] * readout).reshape(
        seq_count, -1
    ) * jax.nn.silu(gate_pre)
    local_sq = jnp.sum(mixed * mixed, axis=1)
    total_sq = lax.psum(local_sq, "tp")
    normed = (mixed * lax.rsqrt(total_sq / SSM_WIDTH + EPS)[:, None] * gain_mix).astype(
        jnp.bfloat16
    )
    products = jnp.dot(
        lax.all_gather(normed, "kv", axis=0, tiled=True), w_out, preferred_element_type=jnp.float32
    )
    mixed_in = lax.psum_scatter(products, "tp", scatter_dimension=1, tiled=True)
    column_count = mixed_in.shape[1]
    residual = lax.dynamic_slice_in_dim(
        stream, lax.axis_index("tp") * column_count, column_count, 1
    )
    hidden = (residual + mixed_in).astype(jnp.bfloat16)
    lifted = (hidden.astype(jnp.float32) * gain_mlp).astype(jnp.bfloat16)
    all_lifted, all_hidden = (
        lax.all_gather(lifted, "dp", axis=0, tiled=True),
        lax.all_gather(hidden, "dp", axis=0, tiled=True),
    )
    whole_rows = all_hidden.astype(jnp.float32)
    row_sq = jnp.sum(whole_rows * whole_rows, axis=1)
    partial_value = jnp.dot(all_lifted, w_up, preferred_element_type=jnp.float32)
    sq_sum = lax.psum(row_sq, ("kv", "tp"))
    shares = lax.psum_scatter(partial_value, ("kv", "tp"), scatter_dimension=1, tiled=True)
    unit_share = jnp.square(jax.nn.relu(shares * lax.rsqrt(sq_sum / D + EPS)[:, None])).astype(
        jnp.bfloat16
    )
    hidden_units = lax.all_gather(unit_share, ("kv", "tp"), axis=1, tiled=True)
    lowered = lax.psum_scatter(
        jnp.dot(hidden_units, w_down, preferred_element_type=jnp.float32),
        "dp",
        scatter_dimension=0,
        tiled=True,
    )
    return (hidden.astype(jnp.float32) + lowered).astype(jnp.bfloat16)


MESH = pl.DeviceIdType.MESH
LANES = 128
F32 = jnp.float32
BF16 = jnp.bfloat16

(
    INPUTS,
    GAIN_IN,
    W_GATE,
    W_INPUT,
    W_BPROJ,
    W_CPROJ,
    W_STEP,
    CONV_INPUT,
    CONV_BPROJ,
    CONV_CPROJ,
    TAIL_INPUT,
    TAIL_BPROJ,
    TAIL_CPROJ,
    STEP_BIAS,
    DECAY_LOG,
    BLOCK_INPUT,
    BLOCK_BPROJ,
    BLOCK_STEP,
    LENGTHS,
    STATE,
    GAIN_MIX,
    W_OUT,
    GAIN_MLP,
    W_UP,
    W_DOWN,
) = NAMES = range(25)
EARLY = (
    INPUTS, GAIN_IN, W_STEP, W_GATE, W_INPUT, W_BPROJ, W_CPROJ,
)
MIDDLE = (
    CONV_INPUT, CONV_BPROJ, CONV_CPROJ, TAIL_INPUT, TAIL_BPROJ, TAIL_CPROJ,
    STEP_BIAS, DECAY_LOG, BLOCK_STEP, BLOCK_BPROJ, BLOCK_INPUT, STATE,
    GAIN_MIX, W_OUT, GAIN_MLP,
)
LATE = (W_UP, W_DOWN)
COPIED = EARLY + MIDDLE + LATE


def send(source, target, send_sem, recv_sem, device):
    copy = pltpu.make_async_remote_copy(
        src_ref=source,
        dst_ref=target,
        send_sem=send_sem,
        recv_sem=recv_sem,
        device_id=device,
        device_id_type=MESH,
    )
    copy.start()
    return copy


def taps(history, weights, newest):
    summed = weights[TAPS - 1 :] * newest
    for offset in range(TAPS - 1):
        summed = summed + weights[offset : offset + 1] * history[offset].astype(F32)
    return summed * lax.logistic(summed)


def fused(sizes, *refs):
    kv, tp, dp = sizes
    hbm = dict(zip(NAMES, refs[: len(NAMES)]))
    out_ref = refs[len(NAMES)]
    rest = list(refs[len(NAMES) + 1 :])
    vm = dict(zip(COPIED, rest[: len(COPIED)]))
    (
        a_send, a_recv, g_buf, p_send, p_recv, h_buf, q_buf, u_send, u_recv, r_send, r_recv, own_sum,
        units, l_send, l_recv,
        local_sem, a_ss, a_rs, g_ss, g_rs, p_ss, p_rs, h_ss, h_rs, q_ss, q_rs, u_ss, u_rs,
        r_ss, r_rs, n_ss, n_rs, f_ss, f_rs, l_ss, l_rs,
    ) = rest[len(COPIED) :]
    me_kv, me_tp, me_dp = lax.axis_index("kv"), lax.axis_index("tp"), lax.axis_index("dp")
    me_unit = me_kv * tp + me_tp

    def kv_peer(j):
        return lax.rem(me_kv + j, kv)

    def tp_peer(q):
        return lax.rem(me_tp + q, tp)

    def dp_peer(d):
        return lax.rem(me_dp + d, dp)

    pairs = [(j, q) for j in range(kv) for q in range(tp) if j or q]
    far_first = sorted(range(kv), key=lambda j: -min(j, kv - j))
    near_first = [j for j in reversed(far_first) if j]

    barrier = pltpu.get_barrier_semaphore()
    for j, q in pairs:
        pl.semaphore_signal(
            barrier, inc=1, device_id={"kv": kv_peer(j), "tp": tp_peer(q)}, device_id_type=MESH
        )
    for d in range(1, dp):
        pl.semaphore_signal(barrier, inc=1, device_id={"dp": dp_peer(d)}, device_id_type=MESH)

    local = {
        name: pltpu.make_async_copy(hbm[name], vm[name], local_sem.at[index])
        for index, name in enumerate(COPIED)
    }
    for name in EARLY:
        local[name].start()
    pending = []

    local[INPUTS].wait()
    local[GAIN_IN].wait()
    stream = vm[INPUTS][...].astype(F32)
    rows = stream.shape[0]
    seqs = rows // kv
    scaled = (stream * vm[GAIN_IN][...]).astype(BF16)
    squares = jnp.sum(stream * stream, axis=1, keepdims=True)
    spans = {}
    at = 0
    for name in (W_GATE, W_INPUT, W_BPROJ, W_CPROJ, W_STEP):
        width = vm[name].shape[name != W_STEP]
        spans[name] = at, at + width
        local[name].wait()
        if name == W_GATE:
            for other in MIDDLE:
                local[other].start()
        piece = lax.dot_general(
            scaled,
            vm[name][...],
            (((1,), (int(name == W_STEP),)), ((), ())),
            preferred_element_type=F32,
        )
        for k in range(kv):
            a_send[k, :, at : at + width] = piece[k * seqs : (k + 1) * seqs]
        at += -(-width // LANES) * LANES
    wide_squares = jnp.broadcast_to(squares, (rows, LANES))
    for k in range(kv):
        a_send[k, :, at : at + LANES] = wide_squares[k * seqs : (k + 1) * seqs]
    for name in LATE:
        local[name].start()
    pl.semaphore_wait(barrier, len(pairs) + dp - 1)
    copies = [
        send(a_send.at[kv_peer(j)], a_recv.at[j - 1], a_ss.at[j - 1], a_rs.at[j - 1], {"kv": kv_peer(j)})
        for j in far_first
        if j
    ]

    for name in MIDDLE[:-3]:
        local[name].wait()
    heads = vm[STEP_BIAS].shape[1]
    groups = vm[W_BPROJ].shape[1] // D_STATE
    per_group = heads // groups
    channels = heads * HEAD_DIM
    block = vm[BLOCK_STEP].shape[2]
    head_eye = lax.broadcasted_iota(jnp.int32, (heads, heads), 0) == lax.broadcasted_iota(
        jnp.int32, (heads, heads), 1
    )

    def column(row):
        return jnp.sum(jnp.where(head_eye, row, 0.0), axis=1, keepdims=True)

    later_than = (
        lax.broadcasted_iota(jnp.int32, (block, block), 0)
        > lax.broadcasted_iota(jnp.int32, (block, block), 1)
    ).astype(F32)
    positions = lax.broadcasted_iota(jnp.int32, (heads, block), 1)
    decay_rate = column(-jnp.exp(vm[DECAY_LOG][...]))
    prepared = []
    for b in range(seqs):
        live = positions < hbm[LENGTHS][b]
        steps = vm[BLOCK_STEP][b]
        masked = jnp.where(live, steps, 0.0)
        later = jnp.dot(
            masked, later_than, precision=lax.Precision.HIGHEST, preferred_element_type=F32
        )
        state = vm[STATE][b].reshape(channels, D_STATE)
        high = state.astype(BF16)
        state_parts = jnp.concatenate([high, (state - high.astype(F32)).astype(BF16)], axis=1)
        prepared.append((live, steps, later, jnp.sum(masked, axis=1, keepdims=True), state_parts))
    own_head = lax.broadcasted_iota(jnp.int32, (heads, channels), 0) == (
        lax.broadcasted_iota(jnp.int32, (heads, channels), 1) // HEAD_DIM
    )
    own_group = (lax.broadcasted_iota(jnp.int32, (heads, groups * D_STATE), 0) // per_group) == (
        lax.broadcasted_iota(jnp.int32, (heads, groups * D_STATE), 1) // D_STATE
    )

    projected = a_send[me_kv]
    for copy, j in zip(copies, [j for j in far_first if j]):
        copy.wait_recv()
        projected = projected + a_recv[j - 1]
    pending += copies
    features = vm[INPUTS].shape[1] * kv
    inverse = lax.rsqrt(projected[:, at : at + 1] / features + EPS)

    def part(name):
        return projected[:, spans[name][0] : spans[name][1]] * inverse

    gate_pre, value_pre, b_pre, c_pre, step_pre = [
        part(name) for name in (W_GATE, W_INPUT, W_BPROJ, W_CPROJ, W_STEP)
    ]
    biased = step_pre + vm[STEP_BIAS][...]
    softened = jnp.maximum(biased, 0.0) + jnp.log1p(jnp.exp(-jnp.abs(biased)))
    mixed_rows = []
    all_current = taps(vm[TAIL_INPUT], vm[CONV_INPUT][...], value_pre)
    all_b = taps(vm[TAIL_BPROJ], vm[CONV_BPROJ][...], b_pre)
    all_c = taps(vm[TAIL_CPROJ], vm[CONV_CPROJ][...], c_pre)
    for b in range(seqs):
        live, steps, later, total_steps, state_parts = prepared[b]
        current, b_now, c_now = all_current[b : b + 1], all_b[b : b + 1], all_c[b : b + 1]
        step_size = column(softened[b : b + 1])
        c_spread = jnp.where(own_group, c_now, 0.0)
        scores = lax.dot_general(
            c_spread.astype(BF16),
            vm[BLOCK_BPROJ][b],
            (((1,), (1,)), ((), ())),
            preferred_element_type=F32,
        )
        decays = jnp.where(live, jnp.exp(decay_rate * (step_size + later)), 0.0)
        weights = (decays * scores * steps).astype(BF16)
        inner = jnp.dot(weights, vm[BLOCK_INPUT][b], preferred_element_type=F32)
        own_score = jnp.sum(c_spread * b_now, axis=1, keepdims=True)
        carried = jnp.exp(decay_rate * (step_size + total_steps))
        c_heads = sum(
            c_spread[:, g * D_STATE : (g + 1) * D_STATE] for g in range(groups)
        )
        c_high = c_heads.astype(BF16)
        c_low = (c_heads - c_high.astype(F32)).astype(BF16)
        both = jnp.concatenate(
            [
                jnp.concatenate([c_high, c_high], axis=1),
                jnp.concatenate([c_low, jnp.zeros_like(c_low)], axis=1),
            ],
            axis=0,
        )
        doubled = lax.dot_general(
            both, state_parts, (((1,), (1,)), ((), ())), preferred_element_type=F32
        )
        readout = doubled[:heads] + doubled[heads:]
        terms = inner + (step_size * own_score) * current + carried * readout
        mixed_rows.append(jnp.sum(jnp.where(own_head, terms, 0.0), axis=0, keepdims=True))
    mixed = jnp.concatenate(mixed_rows, axis=0) * (gate_pre * lax.logistic(gate_pre))
    local[GAIN_MIX].wait()
    g_buf[me_kv, :, :channels] = mixed * vm[GAIN_MIX][...]
    g_buf[me_kv, :, channels:] = jnp.broadcast_to(
        jnp.sum(mixed * mixed, axis=1, keepdims=True), (seqs, LANES)
    )
    copies = [
        send(g_buf.at[me_kv], g_buf.at[me_kv], g_ss.at[j - 1], g_rs.at[j - 1], {"kv": kv_peer(j)})
        for j in far_first
        if j
    ]
    local[W_OUT].wait()
    local[GAIN_MLP].wait()
    for copy in copies:
        copy.wait_recv()
    pending += copies

    gathered = jnp.concatenate([g_buf[k] for k in range(kv)], axis=0)
    unscaled = gathered[:, :channels].astype(BF16)
    share = vm[W_OUT].shape[1] // tp
    for q in range(tp):
        p_send[q, :, :share] = jnp.dot(
            unscaled, vm[W_OUT][:, q * share : (q + 1) * share], preferred_element_type=F32
        )
        p_send[q, :, share:] = gathered[:, channels:]
    copies = [
        send(p_send.at[tp_peer(q)], p_recv.at[q - 1], p_ss.at[q - 1], p_rs.at[q - 1], {"tp": tp_peer(q)})
        for q in range(1, tp)
    ]
    residual = stream[:, :share]
    for q in range(1, tp):
        residual = jnp.where(me_tp == q, stream[:, q * share : (q + 1) * share], residual)
    summed = p_send[me_tp]
    for q, copy in enumerate(copies):
        copy.wait_recv()
        summed = summed + p_recv[q]
    pending += copies
    mixed_in = summed[:, :share] * lax.rsqrt(summed[:, share : share + 1] / (channels * tp) + EPS)
    hidden = (residual + mixed_in).astype(BF16).astype(F32)
    h_buf[me_dp] = hidden
    copies = [
        send(h_buf.at[me_dp], h_buf.at[me_dp], h_ss.at[d - 1], h_rs.at[d - 1], {"dp": dp_peer(d)})
        for d in range(1, dp)
    ]
    local[W_UP].wait()
    for copy in copies:
        copy.wait_recv()
    pending += copies

    whole_rows = jnp.concatenate([h_buf[d] for d in range(dp)], axis=0)
    lifted = (whole_rows * vm[GAIN_MLP][...]).astype(BF16)
    all_rows = rows * dp
    row_eye = lax.broadcasted_iota(jnp.int32, (all_rows, q_buf.shape[2]), 0) == (
        lax.broadcasted_iota(jnp.int32, (all_rows, q_buf.shape[2]), 1)
    )
    row_sq = jnp.sum(whole_rows * whole_rows, axis=1, keepdims=True)
    q_buf[0] = jnp.sum(jnp.where(row_eye, row_sq, 0.0), axis=0, keepdims=True)
    q_copies = [
        send(
            q_buf.at[0],
            q_buf.at[slot],
            q_ss.at[slot - 1],
            q_rs.at[slot - 1],
            {"kv": kv_peer(j), "tp": tp_peer(q)},
        )
        for slot, (j, q) in enumerate(pairs, 1)
    ]
    unit_share = vm[W_UP].shape[1] // (kv * tp)

    def raised(j, q):
        chunk = kv_peer(j) * tp + tp_peer(q)
        columns = pl.ds(pl.multiple_of(chunk * unit_share, LANES), unit_share)
        return jnp.dot(lifted, vm[W_UP][:, columns], preferred_element_type=F32)

    u_copies = {}
    for j in far_first:
        for q in range(1, tp):
            u_send[q - 1, j] = raised(j, q)
            u_copies[j, q] = send(
                u_send.at[q - 1, j],
                u_recv.at[q - 1, j],
                u_ss.at[q - 1, j],
                u_rs.at[q - 1, j],
                {"tp": tp_peer(q)},
            )
    r_copies = {}
    for j in far_first:
        total = raised(j, 0)
        for q in range(1, tp):
            u_copies[j, q].wait_recv()
            total = total + u_recv[q - 1, j]
        if j:
            r_send[j - 1] = total.astype(BF16)
            r_copies[j] = send(
                r_send.at[j - 1], r_recv.at[j - 1], r_ss.at[j - 1], r_rs.at[j - 1], {"kv": kv_peer(j)}
            )
        else:
            own_sum[...] = total
    pending += list(u_copies.values()) + list(r_copies.values()) + q_copies
    sq_row = q_buf[0]
    for slot, copy in enumerate(q_copies, 1):
        copy.wait_recv()
        sq_row = sq_row + q_buf[slot]
    sq_sum = jnp.sum(jnp.where(row_eye, sq_row, 0.0), axis=1, keepdims=True)
    inverse_mlp = lax.rsqrt(sq_sum / features + EPS)
    shares = own_sum[...]
    for j in near_first:
        r_copies[j].wait_recv()
        shares = shares + r_recv[j - 1].astype(F32)
    active = jnp.maximum(shares * inverse_mlp, 0.0)
    units[me_unit] = (active * active).astype(BF16)

    n_copies = {}
    for j in far_first:
        if j:
            n_copies[j] = send(
                units.at[me_unit], units.at[me_unit], n_ss.at[j - 1], n_rs.at[j - 1], {"kv": kv_peer(j)}
            )
    f_copies = {}

    def forward(j):
        for q in range(1, tp):
            chunk = lax.rem(me_kv + kv - j, kv) * tp + me_tp
            f_copies[j, q] = send(
                units.at[chunk], units.at[chunk], f_ss.at[q - 1, j], f_rs.at[q - 1, j], {"tp": tp_peer(q)}
            )

    def lower(j, q):
        chunk = lax.rem(me_kv + kv - j, kv) * tp + lax.rem(me_tp + tp - q, tp)
        span = pl.ds(pl.multiple_of(chunk * unit_share, LANES), unit_share)
        return jnp.dot(units[chunk], vm[W_DOWN][span, :], preferred_element_type=F32)

    forward(0)
    local[W_DOWN].wait()
    lowered = lower(0, 0)
    for q in range(1, tp):
        f_copies[0, q].wait_recv()
        lowered = lowered + lower(0, q)
    for j in near_first:
        n_copies[j].wait_recv()
        forward(j)
        lowered = lowered + lower(j, 0)
    for j in near_first:
        for q in range(1, tp):
            f_copies[j, q].wait_recv()
            lowered = lowered + lower(j, q)
    pending += list(n_copies.values()) + list(f_copies.values())

    for d in range(dp):
        l_send[d] = lowered[d * rows : (d + 1) * rows]
    copies = [
        send(l_send.at[dp_peer(d)], l_recv.at[d - 1], l_ss.at[d - 1], l_rs.at[d - 1], {"dp": dp_peer(d)})
        for d in range(1, dp)
    ]
    for copy in pending:
        copy.wait_send()
    result = h_buf[me_dp] + l_send[me_dp]
    for d, copy in enumerate(copies):
        copy.wait_recv()
        result = result + l_recv[d]
    out_ref[...] = result.astype(BF16)
    for copy in copies:
        copy.wait_send()


def fused_device(sizes, *args):
    kv, tp, dp = sizes
    named = dict(zip(NAMES, args))
    for name in (GAIN_IN, STEP_BIAS, DECAY_LOG, GAIN_MIX, GAIN_MLP):
        named[name] = named[name].reshape(1, -1)
    named[W_STEP] = named[W_STEP].T
    named[BLOCK_STEP] = named[BLOCK_STEP].transpose(0, 2, 1)
    for name in (TAIL_INPUT, TAIL_BPROJ, TAIL_CPROJ):
        named[name] = named[name].transpose(1, 0, 2)
    rows = named[INPUTS].shape[0]
    seqs = rows // kv
    pads = [
        -(-width // LANES) * LANES
        for width in [named[name].shape[1] for name in (W_GATE, W_INPUT, W_BPROJ, W_CPROJ)]
        + [named[W_STEP].shape[0]]
    ]
    wide = sum(pads) + LANES
    channels = named[W_GATE].shape[1]
    share = named[W_OUT].shape[1] // tp
    all_rows = rows * dp
    unit_share = named[W_UP].shape[1] // (kv * tp)
    columns = named[W_DOWN].shape[1]
    row_lanes = -(-all_rows // LANES) * LANES
    dma = pltpu.SemaphoreType.DMA
    scratch = [pltpu.VMEM(named[name].shape, named[name].dtype) for name in COPIED] + [
        pltpu.VMEM((kv, seqs, wide), F32),
        pltpu.VMEM((kv - 1, seqs, wide), F32),
        pltpu.VMEM((kv, seqs, channels + LANES), F32),
        pltpu.VMEM((tp, rows, share + LANES), F32),
        pltpu.VMEM((tp - 1, rows, share + LANES), F32),
        pltpu.VMEM((dp, rows, share), F32),
        pltpu.VMEM((kv * tp, 1, row_lanes), F32),
        pltpu.VMEM((tp - 1, kv, all_rows, unit_share), F32),
        pltpu.VMEM((tp - 1, kv, all_rows, unit_share), F32),
        pltpu.VMEM((kv - 1, all_rows, unit_share), BF16),
        pltpu.VMEM((kv - 1, all_rows, unit_share), BF16),
        pltpu.VMEM((all_rows, unit_share), F32),
        pltpu.VMEM((kv * tp, all_rows, unit_share), BF16),
        pltpu.VMEM((dp, rows, columns), F32),
        pltpu.VMEM((dp - 1, rows, columns), F32),
        dma((len(COPIED),)),
        dma((kv - 1,)), dma((kv - 1,)),
        dma((kv - 1,)), dma((kv - 1,)),
        dma((tp - 1,)), dma((tp - 1,)),
        dma((dp - 1,)), dma((dp - 1,)),
        dma((kv * tp - 1,)), dma((kv * tp - 1,)),
        dma((tp - 1, kv)), dma((tp - 1, kv)),
        dma((kv - 1,)), dma((kv - 1,)),
        dma((kv - 1,)), dma((kv - 1,)),
        dma((tp - 1, kv)), dma((tp - 1, kv)),
        dma((dp - 1,)), dma((dp - 1,)),
    ]
    spaces = [
        pl.BlockSpec(memory_space=pltpu.SMEM if name == LENGTHS else pl.ANY) for name in NAMES
    ]
    return pl.pallas_call(
        functools.partial(fused, sizes),
        out_shape=jax.ShapeDtypeStruct((rows, columns), BF16),
        in_specs=spaces,
        out_specs=pl.BlockSpec(memory_space=pltpu.VMEM),
        scratch_shapes=scratch,
        compiler_params=pltpu.CompilerParams(
            collective_id=0, has_side_effects=True, vmem_limit_bytes=60 * 1024 * 1024
        ),
    )(*[named[name] for name in NAMES])


def choose(sizes, *args):
    kv, tp, _ = sizes
    named = dict(zip(NAMES, args))
    pieces = (named[W_UP].shape[1] // (kv * tp), named[W_OUT].shape[1] // tp)
    if min(sizes) > 1 and all(piece % LANES == 0 for piece in pieces):
        return fused_device(sizes, *args)
    return per_device(*args)


def solution(mesh):
    sizes = tuple(mesh.shape[axis] for axis in ("kv", "tp", "dp"))
    return jax.shard_map(
        functools.partial(choose, sizes),
        mesh=mesh,
        in_specs=(
            P(("grp", "dp"), "kv"),
            P("kv"),
            P("kv", "tp"),
            P("kv", "tp"),
            P("kv", "tp"),
            P("kv", "tp"),
            P("kv", "tp"),
            P(None, "tp"),
            P(None, "tp"),
            P(None, "tp"),
            P(("grp", "dp", "kv"), None, "tp"),
            P(("grp", "dp", "kv"), None, "tp"),
            P(("grp", "dp", "kv"), None, "tp"),
            P("tp"),
            P("tp"),
            P(("grp", "dp", "kv"), None, "tp"),
            P(("grp", "dp", "kv"), None, "tp"),
            P(("grp", "dp", "kv"), None, "tp"),
            P(("grp", "dp", "kv")),
            P(("grp", "dp", "kv"), "tp", None, None),
            P("tp"),
            P("tp", "kv"),
            P(("kv", "tp")),
            P(("kv", "tp"), "dp"),
            P("dp", ("kv", "tp")),
        ),
        out_specs=P(("grp", "dp"), ("kv", "tp")),
        check_vma=False,
    )
```

```python
import functools

import jax
import jax.numpy as jnp
from jax import lax
from jax.experimental import pallas as pl
from jax.experimental.pallas import tpu as pltpu
from jax.sharding import PartitionSpec as P

D = 4096
HEAD_DIM = 64
D_STATE = 128
TAPS = 4
SSM_WIDTH = 2048


EPS = 1e-06


def convolve(history, weights, newest):
    summed = weights[TAPS - 1] * newest
    for offset in range(TAPS - 1):
        summed = summed + weights[offset] * history[:, offset].astype(jnp.float32)
    return jax.nn.silu(summed)


def per_device(
    inputs,
    gain_in,
    w_gate,
    w_input,
    w_bproj,
    w_cproj,
    w_step,
    conv_input,
    conv_bproj,
    conv_cproj,
    tail_input,
    tail_bproj,
    tail_cproj,
    step_bias,
    decay_log,
    block_input,
    block_bproj,
    block_step,
    lengths,
    state,
    gain_mix,
    w_out,
    gain_mlp,
    w_up,
    w_down,
):
    stream = inputs.astype(jnp.float32)
    squares = jnp.sum(stream * stream, axis=1)
    scaled = (stream * gain_in).astype(jnp.bfloat16)
    matrices = (w_gate, w_input, w_bproj, w_cproj, w_step)
    pieces = [jnp.dot(scaled, weight, preferred_element_type=jnp.float32) for weight in matrices]
    projected, totals = (
        lax.psum_scatter(jnp.concatenate(pieces, axis=1), "kv", scatter_dimension=0, tiled=True),
        lax.psum_scatter(squares, "kv", scatter_dimension=0, tiled=True),
    )
    inverse = lax.rsqrt(totals / D + EPS)[:, None]
    bounds = [0]
    for weight in matrices:
        bounds.append(bounds[-1] + weight.shape[1])
    gate_pre, value_pre, b_pre, c_pre, step_pre = [
        projected[:, bounds[member] : bounds[member + 1]] * inverse for member in range(5)
    ]
    seq_count = lengths.shape[0]
    head_count = step_bias.shape[0]
    group_count = w_bproj.shape[1] // D_STATE
    block_len = block_step.shape[1]
    per_group = head_count // group_count
    current = convolve(tail_input, conv_input, value_pre)
    b_now = convolve(tail_bproj, conv_bproj, b_pre)
    c_now = convolve(tail_cproj, conv_cproj, c_pre)
    step_size = jax.nn.softplus(step_pre + step_bias)
    decay_rate = -jnp.exp(decay_log)
    positions = lax.broadcasted_iota(jnp.int32, (1, block_len), 1)
    live_rows = (positions < lengths[:, None]).astype(jnp.float32)
    masked = block_step * live_rows[:, :, None]
    later_steps = jnp.sum(masked, axis=1, keepdims=True) - jnp.cumsum(masked, axis=1)
    decays = jnp.exp(decay_rate * (step_size[:, None, :] + later_steps)) * live_rows[:, :, None]
    c_query = c_now.astype(jnp.bfloat16).reshape(seq_count, group_count, D_STATE)
    keys = block_bproj.reshape(seq_count, block_len, group_count, D_STATE)
    scores = jnp.einsum("bsgn,bgn->bsg", keys, c_query, preferred_element_type=jnp.float32)
    scores = jnp.repeat(scores, per_group, axis=2)
    weights = (decays * scores * block_step).astype(jnp.bfloat16)
    values = block_input.reshape(seq_count, block_len, head_count, HEAD_DIM)
    inner_sum = jnp.einsum("bsh,bshp->bhp", weights, values, preferred_element_type=jnp.float32)
    c_full = c_now.reshape(seq_count, group_count, D_STATE)
    b_full = b_now.reshape(seq_count, group_count, D_STATE)
    own_score = jnp.repeat(jnp.sum(c_full * b_full, axis=2), per_group, axis=1)
    own_term = (step_size * own_score)[:, :, None] * current.reshape(
        seq_count, head_count, HEAD_DIM
    )
    carried = jnp.exp(decay_rate * (step_size + jnp.sum(masked, axis=1)))
    c_heads = jnp.repeat(c_full, per_group, axis=1)
    readout = jnp.einsum("bhpn,bhn->bhp", state, c_heads, precision=lax.Precision.HIGHEST)
    mixed = (inner_sum + own_term + carried[:, :, None] * readout).reshape(
        seq_count, -1
    ) * jax.nn.silu(gate_pre)
    local_sq = jnp.sum(mixed * mixed, axis=1)
    total_sq = lax.psum(local_sq, "tp")
    normed = (mixed * lax.rsqrt(total_sq / SSM_WIDTH + EPS)[:, None] * gain_mix).astype(
        jnp.bfloat16
    )
    products = jnp.dot(
        lax.all_gather(normed, "kv", axis=0, tiled=True), w_out, preferred_element_type=jnp.float32
    )
    mixed_in = lax.psum_scatter(products, "tp", scatter_dimension=1, tiled=True)
    column_count = mixed_in.shape[1]
    residual = lax.dynamic_slice_in_dim(
        stream, lax.axis_index("tp") * column_count, column_count, 1
    )
    hidden = (residual + mixed_in).astype(jnp.bfloat16)
    lifted = (hidden.astype(jnp.float32) * gain_mlp).astype(jnp.bfloat16)
    all_lifted, all_hidden = (
        lax.all_gather(lifted, "dp", axis=0, tiled=True),
        lax.all_gather(hidden, "dp", axis=0, tiled=True),
    )
    whole_rows = all_hidden.astype(jnp.float32)
    row_sq = jnp.sum(whole_rows * whole_rows, axis=1)
    partial_value = jnp.dot(all_lifted, w_up, preferred_element_type=jnp.float32)
    sq_sum = lax.psum(row_sq, ("kv", "tp"))
    shares = lax.psum_scatter(partial_value, ("kv", "tp"), scatter_dimension=1, tiled=True)
    unit_share = jnp.square(jax.nn.relu(shares * lax.rsqrt(sq_sum / D + EPS)[:, None])).astype(
        jnp.bfloat16
    )
    hidden_units = lax.all_gather(unit_share, ("kv", "tp"), axis=1, tiled=True)
    lowered = lax.psum_scatter(
        jnp.dot(hidden_units, w_down, preferred_element_type=jnp.float32),
        "dp",
        scatter_dimension=0,
        tiled=True,
    )
    return (hidden.astype(jnp.float32) + lowered).astype(jnp.bfloat16)


MESH = pl.DeviceIdType.MESH
LANES = 128
F32 = jnp.float32
BF16 = jnp.bfloat16

(
    INPUTS,
    GAIN_IN,
    W_GATE,
    W_INPUT,
    W_BPROJ,
    W_CPROJ,
    W_STEP,
    CONV_INPUT,
    CONV_BPROJ,
    CONV_CPROJ,
    TAIL_INPUT,
    TAIL_BPROJ,
    TAIL_CPROJ,
    STEP_BIAS,
    DECAY_LOG,
    BLOCK_INPUT,
    BLOCK_BPROJ,
    BLOCK_STEP,
    LENGTHS,
    STATE,
    GAIN_MIX,
    W_OUT,
    GAIN_MLP,
    W_UP,
    W_DOWN,
) = NAMES = range(25)
EARLY = (
    INPUTS, GAIN_IN, W_STEP, W_GATE, W_INPUT, W_BPROJ, W_CPROJ,
)
MIDDLE = (
    CONV_INPUT, CONV_BPROJ, CONV_CPROJ, TAIL_INPUT, TAIL_BPROJ, TAIL_CPROJ,
    STEP_BIAS, DECAY_LOG, BLOCK_STEP, BLOCK_BPROJ, BLOCK_INPUT, STATE,
    GAIN_MIX, W_OUT, GAIN_MLP,
)
LATE = (W_UP, W_DOWN)
COPIED = EARLY + MIDDLE + LATE


def send(source, target, send_sem, recv_sem, device):
    copy = pltpu.make_async_remote_copy(
        src_ref=source,
        dst_ref=target,
        send_sem=send_sem,
        recv_sem=recv_sem,
        device_id=device,
        device_id_type=MESH,
    )
    copy.start()
    return copy


def taps(history, weights, newest):
    summed = weights[TAPS - 1 :] * newest
    for offset in range(TAPS - 1):
        summed = summed + weights[offset : offset + 1] * history[offset].astype(F32)
    return summed * lax.logistic(summed)


def fused(sizes, *refs):
    kv, tp, dp = sizes
    hbm = dict(zip(NAMES, refs[: len(NAMES)]))
    out_ref = refs[len(NAMES)]
    rest = list(refs[len(NAMES) + 1 :])
    vm = dict(zip(COPIED, rest[: len(COPIED)]))
    (
        a_send, a_recv, g_buf, p_send, p_recv, h_buf, q_buf, u_send, u_recv, r_send, r_recv, own_sum,
        units, l_send, l_recv, s_send, s_recv, m_buf,
        local_sem, a_ss, a_rs, g_ss, g_rs, p_ss, p_rs, h_ss, h_rs, q_ss, q_rs, u_ss, u_rs,
        r_ss, r_rs, n_ss, n_rs, f_ss, f_rs, l_ss, l_rs, s_ss, s_rs, m_ss, m_rs,
    ) = rest[len(COPIED) :]
    me_kv, me_tp, me_dp = lax.axis_index("kv"), lax.axis_index("tp"), lax.axis_index("dp")
    me_unit = me_kv * tp + me_tp

    def kv_peer(j):
        return lax.rem(me_kv + j, kv)

    def tp_peer(q):
        return lax.rem(me_tp + q, tp)

    def dp_peer(d):
        return lax.rem(me_dp + d, dp)

    pairs = [(j, q) for j in range(kv) for q in range(tp) if j or q]
    far_first = sorted(range(kv), key=lambda j: -min(j, kv - j))
    near_first = [j for j in reversed(far_first) if j]

    barrier = pltpu.get_barrier_semaphore()
    for j, q in pairs:
        pl.semaphore_signal(
            barrier, inc=1, device_id={"kv": kv_peer(j), "tp": tp_peer(q)}, device_id_type=MESH
        )
    for d in range(1, dp):
        pl.semaphore_signal(barrier, inc=1, device_id={"dp": dp_peer(d)}, device_id_type=MESH)

    local = {
        name: pltpu.make_async_copy(hbm[name], vm[name], local_sem.at[index])
        for index, name in enumerate(COPIED)
    }
    for name in EARLY:
        local[name].start()
    pending = []

    local[INPUTS].wait()
    local[GAIN_IN].wait()
    stream = vm[INPUTS][...].astype(F32)
    rows = stream.shape[0]
    seqs = rows // kv
    scaled = (stream * vm[GAIN_IN][...]).astype(BF16)
    squares = jnp.sum(stream * stream, axis=1, keepdims=True)
    spans = {}
    at = 0
    for name in (W_GATE, W_INPUT, W_BPROJ, W_CPROJ, W_STEP):
        width = vm[name].shape[name != W_STEP]
        spans[name] = (at, at + width) if name != W_STEP else (0, width)
        local[name].wait()
        if name == W_GATE:
            for other in MIDDLE:
                local[other].start()
        if name == W_STEP:
            at = 0
        piece = lax.dot_general(
            scaled,
            vm[name][...],
            (((1,), (int(name == W_STEP),)), ((), ())),
            preferred_element_type=F32,
        )
        for k in range(kv):
            if name == W_STEP:
                s_send[k, :, :width] = piece[k * seqs : (k + 1) * seqs]
            else:
                a_send[k, :, at : at + width] = piece[k * seqs : (k + 1) * seqs].astype(BF16)
        at += -(-width // LANES) * LANES
    wide_squares = jnp.broadcast_to(squares, (rows, LANES))
    for k in range(kv):
        s_send[k, :, at : at + LANES] = wide_squares[k * seqs : (k + 1) * seqs]
    for name in LATE:
        local[name].start()
    pl.semaphore_wait(barrier, len(pairs) + dp - 1)
    others = [j for j in far_first if j]
    copies = [
        send(a_send.at[kv_peer(j)], a_recv.at[j - 1], a_ss.at[j - 1], a_rs.at[j - 1], {"kv": kv_peer(j)})
        for j in others
    ]
    s_copies = [
        send(s_send.at[kv_peer(j)], s_recv.at[j - 1], s_ss.at[j - 1], s_rs.at[j - 1], {"kv": kv_peer(j)})
        for j in others
    ]

    for name in MIDDLE[:-3]:
        local[name].wait()
    heads = vm[STEP_BIAS].shape[1]
    groups = vm[W_BPROJ].shape[1] // D_STATE
    per_group = heads // groups
    channels = heads * HEAD_DIM
    block = vm[BLOCK_STEP].shape[2]
    head_eye = lax.broadcasted_iota(jnp.int32, (heads, heads), 0) == lax.broadcasted_iota(
        jnp.int32, (heads, heads), 1
    )

    def column(row):
        return jnp.sum(jnp.where(head_eye, row, 0.0), axis=1, keepdims=True)

    later_than = (
        lax.broadcasted_iota(jnp.int32, (block, block), 0)
        > lax.broadcasted_iota(jnp.int32, (block, block), 1)
    ).astype(F32)
    positions = lax.broadcasted_iota(jnp.int32, (heads, block), 1)
    decay_rate = column(-jnp.exp(vm[DECAY_LOG][...]))
    prepared = []
    for b in range(seqs):
        live = positions < hbm[LENGTHS][b]
        steps = vm[BLOCK_STEP][b]
        masked = jnp.where(live, steps, 0.0)
        later = jnp.dot(
            masked, later_than, precision=lax.Precision.HIGHEST, preferred_element_type=F32
        )
        state = vm[STATE][b].reshape(channels, D_STATE)
        high = state.astype(BF16)
        state_parts = jnp.concatenate([high, (state - high.astype(F32)).astype(BF16)], axis=1)
        prepared.append((live, steps, later, jnp.sum(masked, axis=1, keepdims=True), state_parts))
    own_head = lax.broadcasted_iota(jnp.int32, (heads, channels), 0) == (
        lax.broadcasted_iota(jnp.int32, (heads, channels), 1) // HEAD_DIM
    )
    own_group = (lax.broadcasted_iota(jnp.int32, (heads, groups * D_STATE), 0) // per_group) == (
        lax.broadcasted_iota(jnp.int32, (heads, groups * D_STATE), 1) // D_STATE
    )

    projected = a_send[me_kv].astype(F32)
    stepped = s_send[me_kv]
    for copy, s_copy, j in zip(copies, s_copies, others):
        copy.wait_recv()
        s_copy.wait_recv()
        projected = projected + a_recv[j - 1].astype(F32)
        stepped = stepped + s_recv[j - 1]
    pending += copies + s_copies
    features = vm[INPUTS].shape[1] * kv
    inverse = lax.rsqrt(stepped[:, at : at + 1] / features + EPS)

    def part(name):
        source = stepped if name == W_STEP else projected
        return source[:, spans[name][0] : spans[name][1]] * inverse

    gate_pre, value_pre, b_pre, c_pre, step_pre = [
        part(name) for name in (W_GATE, W_INPUT, W_BPROJ, W_CPROJ, W_STEP)
    ]
    biased = step_pre + vm[STEP_BIAS][...]
    softened = jnp.maximum(biased, 0.0) + jnp.log1p(jnp.exp(-jnp.abs(biased)))
    mixed_rows = []
    all_current = taps(vm[TAIL_INPUT], vm[CONV_INPUT][...], value_pre)
    all_b = taps(vm[TAIL_BPROJ], vm[CONV_BPROJ][...], b_pre)
    all_c = taps(vm[TAIL_CPROJ], vm[CONV_CPROJ][...], c_pre)
    for b in range(seqs):
        live, steps, later, total_steps, state_parts = prepared[b]
        current, b_now, c_now = all_current[b : b + 1], all_b[b : b + 1], all_c[b : b + 1]
        step_size = column(softened[b : b + 1])
        c_spread = jnp.where(own_group, c_now, 0.0)
        scores = lax.dot_general(
            c_spread.astype(BF16),
            vm[BLOCK_BPROJ][b],
            (((1,), (1,)), ((), ())),
            preferred_element_type=F32,
        )
        decays = jnp.where(live, jnp.exp(decay_rate * (step_size + later)), 0.0)
        weights = (decays * scores * steps).astype(BF16)
        inner = jnp.dot(weights, vm[BLOCK_INPUT][b], preferred_element_type=F32)
        own_score = jnp.sum(c_spread * b_now, axis=1, keepdims=True)
        carried = jnp.exp(decay_rate * (step_size + total_steps))
        c_heads = sum(
            c_spread[:, g * D_STATE : (g + 1) * D_STATE] for g in range(groups)
        )
        c_high = c_heads.astype(BF16)
        c_low = (c_heads - c_high.astype(F32)).astype(BF16)
        both = jnp.concatenate(
            [
                jnp.concatenate([c_high, c_high], axis=1),
                jnp.concatenate([c_low, jnp.zeros_like(c_low)], axis=1),
            ],
            axis=0,
        )
        doubled = lax.dot_general(
            both, state_parts, (((1,), (1,)), ((), ())), preferred_element_type=F32
        )
        readout = doubled[:heads] + doubled[heads:]
        terms = inner + (step_size * own_score) * current + carried * readout
        mixed_rows.append(jnp.sum(jnp.where(own_head, terms, 0.0), axis=0, keepdims=True))
    mixed = jnp.concatenate(mixed_rows, axis=0) * (gate_pre * lax.logistic(gate_pre))
    local[GAIN_MIX].wait()
    g_buf[me_kv] = (mixed * vm[GAIN_MIX][...]).astype(BF16)
    m_buf[me_kv] = jnp.broadcast_to(
        jnp.sum(mixed * mixed, axis=1, keepdims=True), (seqs, LANES)
    )
    copies = [
        send(g_buf.at[me_kv], g_buf.at[me_kv], g_ss.at[j - 1], g_rs.at[j - 1], {"kv": kv_peer(j)})
        for j in others
    ] + [
        send(m_buf.at[me_kv], m_buf.at[me_kv], m_ss.at[j - 1], m_rs.at[j - 1], {"kv": kv_peer(j)})
        for j in others
    ]
    local[W_OUT].wait()
    local[GAIN_MLP].wait()
    for copy in copies:
        copy.wait_recv()
    pending += copies

    unscaled = jnp.concatenate([g_buf[k].astype(F32) for k in range(kv)], axis=0).astype(BF16)
    partial_sq = jnp.concatenate([m_buf[k] for k in range(kv)], axis=0)
    share = vm[W_OUT].shape[1] // tp

    def product(q):
        start = pl.multiple_of(tp_peer(q) * share, LANES)
        return jnp.dot(unscaled, vm[W_OUT][:, pl.ds(start, share)], preferred_element_type=F32)

    copies = []
    for q in range(1, tp):
        p_send[q - 1, :, :share] = product(q)
        p_send[q - 1, :, share:] = partial_sq
        copies.append(
            send(p_send.at[q - 1], p_recv.at[q - 1], p_ss.at[q - 1], p_rs.at[q - 1], {"tp": tp_peer(q)})
        )
    summed = product(0)
    residual = stream[:, :share]
    for q in range(1, tp):
        residual = jnp.where(me_tp == q, stream[:, q * share : (q + 1) * share], residual)
    total_sq = partial_sq[:, :1]
    for q, copy in enumerate(copies):
        copy.wait_recv()
        summed = summed + p_recv[q, :, :share]
        total_sq = total_sq + p_recv[q, :, share : share + 1]
    pending += copies
    mixed_in = summed * lax.rsqrt(total_sq / (channels * tp) + EPS)
    hidden = (residual + mixed_in).astype(BF16).astype(F32)
    h_buf[me_dp] = hidden
    copies = [
        send(h_buf.at[me_dp], h_buf.at[me_dp], h_ss.at[d - 1], h_rs.at[d - 1], {"dp": dp_peer(d)})
        for d in range(1, dp)
    ]
    local[W_UP].wait()
    for copy in copies:
        copy.wait_recv()
    pending += copies

    whole_rows = jnp.concatenate([h_buf[d] for d in range(dp)], axis=0)
    lifted = (whole_rows * vm[GAIN_MLP][...]).astype(BF16)
    all_rows = rows * dp
    row_eye = lax.broadcasted_iota(jnp.int32, (all_rows, q_buf.shape[2]), 0) == (
        lax.broadcasted_iota(jnp.int32, (all_rows, q_buf.shape[2]), 1)
    )
    row_sq = jnp.sum(whole_rows * whole_rows, axis=1, keepdims=True)
    q_buf[0] = jnp.sum(jnp.where(row_eye, row_sq, 0.0), axis=0, keepdims=True)
    q_copies = [
        send(
            q_buf.at[0],
            q_buf.at[slot],
            q_ss.at[slot - 1],
            q_rs.at[slot - 1],
            {"kv": kv_peer(j), "tp": tp_peer(q)},
        )
        for slot, (j, q) in enumerate(pairs, 1)
    ]
    unit_share = vm[W_UP].shape[1] // (kv * tp)

    def raised(j, q):
        chunk = kv_peer(j) * tp + tp_peer(q)
        columns = pl.ds(pl.multiple_of(chunk * unit_share, LANES), unit_share)
        return jnp.dot(lifted, vm[W_UP][:, columns], preferred_element_type=F32)

    u_copies, r_copies = {}, {}

    def for_partner(j):
        for q in range(1, tp):
            u_send[q - 1, j] = raised(j, q)
            u_copies[j, q] = send(
                u_send.at[q - 1, j],
                u_recv.at[q - 1, j],
                u_ss.at[q - 1, j],
                u_rs.at[q - 1, j],
                {"tp": tp_peer(q)},
            )

    def for_chip(j):
        total = raised(j, 0)
        for q in range(1, tp):
            u_copies[j, q].wait_recv()
            total = total + u_recv[q - 1, j]
        if j:
            r_send[j - 1] = total.astype(BF16)
            r_copies[j] = send(
                r_send.at[j - 1], r_recv.at[j - 1], r_ss.at[j - 1], r_rs.at[j - 1], {"kv": kv_peer(j)}
            )
        else:
            own_sum[...] = total

    for_partner(far_first[0])
    for earlier, j in zip(far_first, far_first[1:]):
        if j:
            for_partner(j)
            for_chip(earlier)
        else:
            for_chip(earlier)
            for_partner(j)
    for_chip(0)
    pending += list(u_copies.values()) + list(r_copies.values()) + q_copies
    sq_row = q_buf[0]
    for slot, copy in enumerate(q_copies, 1):
        copy.wait_recv()
        sq_row = sq_row + q_buf[slot]
    sq_sum = jnp.sum(jnp.where(row_eye, sq_row, 0.0), axis=1, keepdims=True)
    inverse_mlp = lax.rsqrt(sq_sum / features + EPS)
    shares = own_sum[...]
    for j in near_first:
        r_copies[j].wait_recv()
        shares = shares + r_recv[j - 1].astype(F32)
    active = jnp.maximum(shares * inverse_mlp, 0.0)
    units[me_unit] = (active * active).astype(BF16)

    n_copies = {}
    for j in far_first:
        if j:
            n_copies[j] = send(
                units.at[me_unit], units.at[me_unit], n_ss.at[j - 1], n_rs.at[j - 1], {"kv": kv_peer(j)}
            )
    f_copies = {}

    def forward(j):
        for q in range(1, tp):
            chunk = lax.rem(me_kv + kv - j, kv) * tp + me_tp
            f_copies[j, q] = send(
                units.at[chunk], units.at[chunk], f_ss.at[q - 1, j], f_rs.at[q - 1, j], {"tp": tp_peer(q)}
            )

    def lower(j, q):
        chunk = lax.rem(me_kv + kv - j, kv) * tp + lax.rem(me_tp + tp - q, tp)
        span = pl.ds(pl.multiple_of(chunk * unit_share, LANES), unit_share)
        return jnp.dot(units[chunk], vm[W_DOWN][span, :], preferred_element_type=F32)

    forward(0)
    local[W_DOWN].wait()
    lowered = lower(0, 0)
    for q in range(1, tp):
        f_copies[0, q].wait_recv()
        lowered = lowered + lower(0, q)
    for j in near_first:
        n_copies[j].wait_recv()
        forward(j)
        lowered = lowered + lower(j, 0)
    for j in near_first:
        for q in range(1, tp):
            f_copies[j, q].wait_recv()
            lowered = lowered + lower(j, q)
    pending += list(n_copies.values()) + list(f_copies.values())

    for d in range(dp):
        l_send[d] = lowered[d * rows : (d + 1) * rows]
    copies = [
        send(l_send.at[dp_peer(d)], l_recv.at[d - 1], l_ss.at[d - 1], l_rs.at[d - 1], {"dp": dp_peer(d)})
        for d in range(1, dp)
    ]
    for copy in pending:
        copy.wait_send()
    result = h_buf[me_dp] + l_send[me_dp]
    for d, copy in enumerate(copies):
        copy.wait_recv()
        result = result + l_recv[d]
    out_ref[...] = result.astype(BF16)
    for copy in copies:
        copy.wait_send()


def fused_device(sizes, *args):
    kv, tp, dp = sizes
    named = dict(zip(NAMES, args))
    for name in (GAIN_IN, STEP_BIAS, DECAY_LOG, GAIN_MIX, GAIN_MLP):
        named[name] = named[name].reshape(1, -1)
    named[W_STEP] = named[W_STEP].T
    named[BLOCK_STEP] = named[BLOCK_STEP].transpose(0, 2, 1)
    for name in (TAIL_INPUT, TAIL_BPROJ, TAIL_CPROJ):
        named[name] = named[name].transpose(1, 0, 2)
    rows = named[INPUTS].shape[0]
    seqs = rows // kv
    pads = [
        -(-width // LANES) * LANES
        for width in [named[name].shape[1] for name in (W_GATE, W_INPUT, W_BPROJ, W_CPROJ)]
        + [named[W_STEP].shape[0]]
    ]
    wide, narrow = sum(pads[:-1]), pads[-1] + LANES
    channels = named[W_GATE].shape[1]
    share = named[W_OUT].shape[1] // tp
    all_rows = rows * dp
    unit_share = named[W_UP].shape[1] // (kv * tp)
    columns = named[W_DOWN].shape[1]
    row_lanes = -(-all_rows // LANES) * LANES
    dma = pltpu.SemaphoreType.DMA
    scratch = [pltpu.VMEM(named[name].shape, named[name].dtype) for name in COPIED] + [
        pltpu.VMEM((kv, seqs, wide), BF16),
        pltpu.VMEM((kv - 1, seqs, wide), BF16),
        pltpu.VMEM((kv, seqs, channels), BF16),
        pltpu.VMEM((tp - 1, rows, share + LANES), F32),
        pltpu.VMEM((tp - 1, rows, share + LANES), F32),
        pltpu.VMEM((dp, rows, share), F32),
        pltpu.VMEM((kv * tp, 1, row_lanes), F32),
        pltpu.VMEM((tp - 1, kv, all_rows, unit_share), F32),
        pltpu.VMEM((tp - 1, kv, all_rows, unit_share), F32),
        pltpu.VMEM((kv - 1, all_rows, unit_share), BF16),
        pltpu.VMEM((kv - 1, all_rows, unit_share), BF16),
        pltpu.VMEM((all_rows, unit_share), F32),
        pltpu.VMEM((kv * tp, all_rows, unit_share), BF16),
        pltpu.VMEM((dp, rows, columns), F32),
        pltpu.VMEM((dp - 1, rows, columns), F32),
        pltpu.VMEM((kv, seqs, narrow), F32),
        pltpu.VMEM((kv - 1, seqs, narrow), F32),
        pltpu.VMEM((kv, seqs, LANES), F32),
        dma((len(COPIED),)),
        dma((kv - 1,)), dma((kv - 1,)),
        dma((kv - 1,)), dma((kv - 1,)),
        dma((tp - 1,)), dma((tp - 1,)),
        dma((dp - 1,)), dma((dp - 1,)),
        dma((kv * tp - 1,)), dma((kv * tp - 1,)),
        dma((tp - 1, kv)), dma((tp - 1, kv)),
        dma((kv - 1,)), dma((kv - 1,)),
        dma((kv - 1,)), dma((kv - 1,)),
        dma((tp - 1, kv)), dma((tp - 1, kv)),
        dma((dp - 1,)), dma((dp - 1,)),
        dma((kv - 1,)), dma((kv - 1,)),
        dma((kv - 1,)), dma((kv - 1,)),
    ]
    spaces = [
        pl.BlockSpec(memory_space=pltpu.SMEM if name == LENGTHS else pl.ANY) for name in NAMES
    ]
    return pl.pallas_call(
        functools.partial(fused, sizes),
        out_shape=jax.ShapeDtypeStruct((rows, columns), BF16),
        in_specs=spaces,
        out_specs=pl.BlockSpec(memory_space=pltpu.VMEM),
        scratch_shapes=scratch,
        compiler_params=pltpu.CompilerParams(
            collective_id=0, has_side_effects=True, vmem_limit_bytes=60 * 1024 * 1024
        ),
    )(*[named[name] for name in NAMES])


def choose(sizes, *args):
    kv, tp, _ = sizes
    named = dict(zip(NAMES, args))
    pieces = (named[W_UP].shape[1] // (kv * tp), named[W_OUT].shape[1] // tp)
    if min(sizes) > 1 and all(piece % LANES == 0 for piece in pieces):
        return fused_device(sizes, *args)
    return per_device(*args)


def solution(mesh):
    sizes = tuple(mesh.shape[axis] for axis in ("kv", "tp", "dp"))
    return jax.shard_map(
        functools.partial(choose, sizes),
        mesh=mesh,
        in_specs=(
            P(("grp", "dp"), "kv"),
            P("kv"),
            P("kv", "tp"),
            P("kv", "tp"),
            P("kv", "tp"),
            P("kv", "tp"),
            P("kv", "tp"),
            P(None, "tp"),
            P(None, "tp"),
            P(None, "tp"),
            P(("grp", "dp", "kv"), None, "tp"),
            P(("grp", "dp", "kv"), None, "tp"),
            P(("grp", "dp", "kv"), None, "tp"),
            P("tp"),
            P("tp"),
            P(("grp", "dp", "kv"), None, "tp"),
            P(("grp", "dp", "kv"), None, "tp"),
            P(("grp", "dp", "kv"), None, "tp"),
            P(("grp", "dp", "kv")),
            P(("grp", "dp", "kv"), "tp", None, None),
            P("tp"),
            P("tp", "kv"),
            P(("kv", "tp")),
            P(("kv", "tp"), "dp"),
            P("dp", ("kv", "tp")),
        ),
        out_specs=P(("grp", "dp"), ("kv", "tp")),
        check_vma=False,
    )
```

```python
import functools

import jax
import jax.numpy as jnp
from jax import lax
from jax.experimental import pallas as pl
from jax.experimental.pallas import tpu as pltpu
from jax.sharding import PartitionSpec as P

D = 4096
HEAD_DIM = 64
D_STATE = 128
TAPS = 4
SSM_WIDTH = 2048


EPS = 1e-06


def convolve(history, weights, newest):
    summed = weights[TAPS - 1] * newest
    for offset in range(TAPS - 1):
        summed = summed + weights[offset] * history[:, offset].astype(jnp.float32)
    return jax.nn.silu(summed)


def per_device(
    inputs,
    gain_in,
    w_gate,
    w_input,
    w_bproj,
    w_cproj,
    w_step,
    conv_input,
    conv_bproj,
    conv_cproj,
    tail_input,
    tail_bproj,
    tail_cproj,
    step_bias,
    decay_log,
    block_input,
    block_bproj,
    block_step,
    lengths,
    state,
    gain_mix,
    w_out,
    gain_mlp,
    w_up,
    w_down,
):
    stream = inputs.astype(jnp.float32)
    squares = jnp.sum(stream * stream, axis=1)
    scaled = (stream * gain_in).astype(jnp.bfloat16)
    matrices = (w_gate, w_input, w_bproj, w_cproj, w_step)
    pieces = [jnp.dot(scaled, weight, preferred_element_type=jnp.float32) for weight in matrices]
    projected, totals = (
        lax.psum_scatter(jnp.concatenate(pieces, axis=1), "kv", scatter_dimension=0, tiled=True),
        lax.psum_scatter(squares, "kv", scatter_dimension=0, tiled=True),
    )
    inverse = lax.rsqrt(totals / D + EPS)[:, None]
    bounds = [0]
    for weight in matrices:
        bounds.append(bounds[-1] + weight.shape[1])
    gate_pre, value_pre, b_pre, c_pre, step_pre = [
        projected[:, bounds[member] : bounds[member + 1]] * inverse for member in range(5)
    ]
    seq_count = lengths.shape[0]
    head_count = step_bias.shape[0]
    group_count = w_bproj.shape[1] // D_STATE
    block_len = block_step.shape[1]
    per_group = head_count // group_count
    current = convolve(tail_input, conv_input, value_pre)
    b_now = convolve(tail_bproj, conv_bproj, b_pre)
    c_now = convolve(tail_cproj, conv_cproj, c_pre)
    step_size = jax.nn.softplus(step_pre + step_bias)
    decay_rate = -jnp.exp(decay_log)
    positions = lax.broadcasted_iota(jnp.int32, (1, block_len), 1)
    live_rows = (positions < lengths[:, None]).astype(jnp.float32)
    masked = block_step * live_rows[:, :, None]
    later_steps = jnp.sum(masked, axis=1, keepdims=True) - jnp.cumsum(masked, axis=1)
    decays = jnp.exp(decay_rate * (step_size[:, None, :] + later_steps)) * live_rows[:, :, None]
    c_query = c_now.astype(jnp.bfloat16).reshape(seq_count, group_count, D_STATE)
    keys = block_bproj.reshape(seq_count, block_len, group_count, D_STATE)
    scores = jnp.einsum("bsgn,bgn->bsg", keys, c_query, preferred_element_type=jnp.float32)
    scores = jnp.repeat(scores, per_group, axis=2)
    weights = (decays * scores * block_step).astype(jnp.bfloat16)
    values = block_input.reshape(seq_count, block_len, head_count, HEAD_DIM)
    inner_sum = jnp.einsum("bsh,bshp->bhp", weights, values, preferred_element_type=jnp.float32)
    c_full = c_now.reshape(seq_count, group_count, D_STATE)
    b_full = b_now.reshape(seq_count, group_count, D_STATE)
    own_score = jnp.repeat(jnp.sum(c_full * b_full, axis=2), per_group, axis=1)
    own_term = (step_size * own_score)[:, :, None] * current.reshape(
        seq_count, head_count, HEAD_DIM
    )
    carried = jnp.exp(decay_rate * (step_size + jnp.sum(masked, axis=1)))
    c_heads = jnp.repeat(c_full, per_group, axis=1)
    readout = jnp.einsum("bhpn,bhn->bhp", state, c_heads, precision=lax.Precision.HIGHEST)
    mixed = (inner_sum + own_term + carried[:, :, None] * readout).reshape(
        seq_count, -1
    ) * jax.nn.silu(gate_pre)
    local_sq = jnp.sum(mixed * mixed, axis=1)
    total_sq = lax.psum(local_sq, "tp")
    normed = (mixed * lax.rsqrt(total_sq / SSM_WIDTH + EPS)[:, None] * gain_mix).astype(
        jnp.bfloat16
    )
    products = jnp.dot(
        lax.all_gather(normed, "kv", axis=0, tiled=True), w_out, preferred_element_type=jnp.float32
    )
    mixed_in = lax.psum_scatter(products, "tp", scatter_dimension=1, tiled=True)
    column_count = mixed_in.shape[1]
    residual = lax.dynamic_slice_in_dim(
        stream, lax.axis_index("tp") * column_count, column_count, 1
    )
    hidden = (residual + mixed_in).astype(jnp.bfloat16)
    lifted = (hidden.astype(jnp.float32) * gain_mlp).astype(jnp.bfloat16)
    all_lifted, all_hidden = (
        lax.all_gather(lifted, "dp", axis=0, tiled=True),
        lax.all_gather(hidden, "dp", axis=0, tiled=True),
    )
    whole_rows = all_hidden.astype(jnp.float32)
    row_sq = jnp.sum(whole_rows * whole_rows, axis=1)
    partial_value = jnp.dot(all_lifted, w_up, preferred_element_type=jnp.float32)
    sq_sum = lax.psum(row_sq, ("kv", "tp"))
    shares = lax.psum_scatter(partial_value, ("kv", "tp"), scatter_dimension=1, tiled=True)
    unit_share = jnp.square(jax.nn.relu(shares * lax.rsqrt(sq_sum / D + EPS)[:, None])).astype(
        jnp.bfloat16
    )
    hidden_units = lax.all_gather(unit_share, ("kv", "tp"), axis=1, tiled=True)
    lowered = lax.psum_scatter(
        jnp.dot(hidden_units, w_down, preferred_element_type=jnp.float32),
        "dp",
        scatter_dimension=0,
        tiled=True,
    )
    return (hidden.astype(jnp.float32) + lowered).astype(jnp.bfloat16)


MESH = pl.DeviceIdType.MESH
LANES = 128
F32 = jnp.float32
BF16 = jnp.bfloat16

(
    INPUTS,
    GAIN_IN,
    W_GATE,
    W_INPUT,
    W_BPROJ,
    W_CPROJ,
    W_STEP,
    CONV_INPUT,
    CONV_BPROJ,
    CONV_CPROJ,
    TAIL_INPUT,
    TAIL_BPROJ,
    TAIL_CPROJ,
    STEP_BIAS,
    DECAY_LOG,
    BLOCK_INPUT,
    BLOCK_BPROJ,
    BLOCK_STEP,
    LENGTHS,
    STATE,
    GAIN_MIX,
    W_OUT,
    GAIN_MLP,
    W_UP,
    W_DOWN,
) = NAMES = range(25)
EARLY = (
    INPUTS, GAIN_IN, W_STEP, W_GATE, W_INPUT, W_BPROJ, W_CPROJ,
)
MIDDLE = (
    CONV_INPUT, CONV_BPROJ, CONV_CPROJ, TAIL_INPUT, TAIL_BPROJ, TAIL_CPROJ,
    STEP_BIAS, DECAY_LOG, BLOCK_STEP, BLOCK_BPROJ, BLOCK_INPUT, STATE,
    GAIN_MIX, W_OUT, GAIN_MLP,
)
LATE = (W_UP, W_DOWN)
COPIED = EARLY + MIDDLE + LATE


def send(source, target, send_sem, recv_sem, device):
    copy = pltpu.make_async_remote_copy(
        src_ref=source,
        dst_ref=target,
        send_sem=send_sem,
        recv_sem=recv_sem,
        device_id=device,
        device_id_type=MESH,
    )
    copy.start()
    return copy


def taps(history, weights, newest):
    summed = weights[TAPS - 1 :] * newest
    for offset in range(TAPS - 1):
        summed = summed + weights[offset : offset + 1] * history[offset].astype(F32)
    return summed * lax.logistic(summed)


def fused(sizes, *refs):
    kv, tp, dp = sizes
    hbm = dict(zip(NAMES, refs[: len(NAMES)]))
    out_ref = refs[len(NAMES)]
    rest = list(refs[len(NAMES) + 1 :])
    vm = dict(zip(COPIED, rest[: len(COPIED)]))
    (
        a_send, a_recv, g_buf, p_send, p_recv, h_buf, q_buf, u_send, u_recv, r_send, r_recv, own_sum,
        units, l_send, l_recv, s_send, s_recv, m_buf,
        local_sem, a_ss, a_rs, g_ss, g_rs, p_ss, p_rs, h_ss, h_rs, q_ss, q_rs, u_ss, u_rs,
        r_ss, r_rs, n_ss, n_rs, f_ss, f_rs, l_ss, l_rs, s_ss, s_rs, m_ss, m_rs,
    ) = rest[len(COPIED) :]
    me_kv, me_tp, me_dp = lax.axis_index("kv"), lax.axis_index("tp"), lax.axis_index("dp")
    me_unit = me_kv * tp + me_tp

    def kv_peer(j):
        return lax.rem(me_kv + j, kv)

    def tp_peer(q):
        return lax.rem(me_tp + q, tp)

    def dp_peer(d):
        return lax.rem(me_dp + d, dp)

    pairs = [(j, q) for j in range(kv) for q in range(tp) if j or q]
    far_first = sorted(range(kv), key=lambda j: -min(j, kv - j))
    near_first = [j for j in reversed(far_first) if j]

    barrier = pltpu.get_barrier_semaphore()
    for j, q in pairs:
        pl.semaphore_signal(
            barrier, inc=1, device_id={"kv": kv_peer(j), "tp": tp_peer(q)}, device_id_type=MESH
        )
    for d in range(1, dp):
        pl.semaphore_signal(barrier, inc=1, device_id={"dp": dp_peer(d)}, device_id_type=MESH)

    local = {
        name: pltpu.make_async_copy(hbm[name], vm[name], local_sem.at[index])
        for index, name in enumerate(COPIED)
    }
    for name in EARLY:
        local[name].start()
    pending = []

    local[INPUTS].wait()
    local[GAIN_IN].wait()
    stream = vm[INPUTS][...].astype(F32)
    rows = stream.shape[0]
    seqs = rows // kv
    scaled = (stream * vm[GAIN_IN][...]).astype(BF16)
    squares = jnp.sum(stream * stream, axis=1, keepdims=True)
    spans = {}
    at = 0
    for name in (W_GATE, W_INPUT, W_BPROJ, W_CPROJ, W_STEP):
        width = vm[name].shape[name != W_STEP]
        spans[name] = (at, at + width) if name != W_STEP else (0, width)
        local[name].wait()
        if name == W_GATE:
            for other in MIDDLE:
                local[other].start()
        if name == W_STEP:
            at = 0
        piece = lax.dot_general(
            scaled,
            vm[name][...],
            (((1,), (int(name == W_STEP),)), ((), ())),
            preferred_element_type=F32,
        )
        for k in range(kv):
            if name == W_STEP:
                s_send[k, :, :width] = piece[k * seqs : (k + 1) * seqs]
            else:
                a_send[k, :, at : at + width] = piece[k * seqs : (k + 1) * seqs].astype(BF16)
        at += -(-width // LANES) * LANES
    wide_squares = jnp.broadcast_to(squares, (rows, LANES))
    for k in range(kv):
        s_send[k, :, at : at + LANES] = wide_squares[k * seqs : (k + 1) * seqs]
    for name in LATE:
        local[name].start()
    pl.semaphore_wait(barrier, len(pairs) + dp - 1)
    others = [j for j in far_first if j]
    copies = [
        send(a_send.at[kv_peer(j)], a_recv.at[j - 1], a_ss.at[j - 1], a_rs.at[j - 1], {"kv": kv_peer(j)})
        for j in others
    ]
    s_copies = [
        send(s_send.at[kv_peer(j)], s_recv.at[j - 1], s_ss.at[j - 1], s_rs.at[j - 1], {"kv": kv_peer(j)})
        for j in others
    ]

    for name in MIDDLE[:-3]:
        local[name].wait()
    heads = vm[STEP_BIAS].shape[1]
    groups = vm[W_BPROJ].shape[1] // D_STATE
    per_group = heads // groups
    channels = heads * HEAD_DIM
    block = vm[BLOCK_STEP].shape[2]
    head_eye = lax.broadcasted_iota(jnp.int32, (heads, heads), 0) == lax.broadcasted_iota(
        jnp.int32, (heads, heads), 1
    )

    def column(row):
        return jnp.sum(jnp.where(head_eye, row, 0.0), axis=1, keepdims=True)

    later_than = (
        lax.broadcasted_iota(jnp.int32, (block, block), 0)
        > lax.broadcasted_iota(jnp.int32, (block, block), 1)
    ).astype(F32)
    positions = lax.broadcasted_iota(jnp.int32, (heads, block), 1)
    decay_rate = column(-jnp.exp(vm[DECAY_LOG][...]))
    prepared = []
    for b in range(seqs):
        live = positions < hbm[LENGTHS][b]
        steps = vm[BLOCK_STEP][b]
        masked = jnp.where(live, steps, 0.0)
        later = jnp.dot(
            masked, later_than, precision=lax.Precision.HIGHEST, preferred_element_type=F32
        )
        state = vm[STATE][b].reshape(channels, D_STATE)
        high = state.astype(BF16)
        state_parts = jnp.concatenate([high, (state - high.astype(F32)).astype(BF16)], axis=1)
        prepared.append((live, steps, later, jnp.sum(masked, axis=1, keepdims=True), state_parts))
    own_head = lax.broadcasted_iota(jnp.int32, (heads, channels), 0) == (
        lax.broadcasted_iota(jnp.int32, (heads, channels), 1) // HEAD_DIM
    )
    own_group = (lax.broadcasted_iota(jnp.int32, (heads, groups * D_STATE), 0) // per_group) == (
        lax.broadcasted_iota(jnp.int32, (heads, groups * D_STATE), 1) // D_STATE
    )

    projected = a_send[me_kv].astype(F32)
    stepped = s_send[me_kv]
    for copy, s_copy, j in zip(copies, s_copies, others):
        copy.wait_recv()
        s_copy.wait_recv()
        projected = projected + a_recv[j - 1].astype(F32)
        stepped = stepped + s_recv[j - 1]
    pending += copies + s_copies
    features = vm[INPUTS].shape[1] * kv
    inverse = lax.rsqrt(stepped[:, at : at + 1] / features + EPS)

    def part(name):
        source = stepped if name == W_STEP else projected
        return source[:, spans[name][0] : spans[name][1]] * inverse

    gate_pre, value_pre, b_pre, c_pre, step_pre = [
        part(name) for name in (W_GATE, W_INPUT, W_BPROJ, W_CPROJ, W_STEP)
    ]
    biased = step_pre + vm[STEP_BIAS][...]
    softened = jnp.maximum(biased, 0.0) + jnp.log1p(jnp.exp(-jnp.abs(biased)))
    mixed_rows = []
    all_current = taps(vm[TAIL_INPUT], vm[CONV_INPUT][...], value_pre)
    all_b = taps(vm[TAIL_BPROJ], vm[CONV_BPROJ][...], b_pre)
    all_c = taps(vm[TAIL_CPROJ], vm[CONV_CPROJ][...], c_pre)
    for b in range(seqs):
        live, steps, later, total_steps, state_parts = prepared[b]
        current, b_now, c_now = all_current[b : b + 1], all_b[b : b + 1], all_c[b : b + 1]
        step_size = column(softened[b : b + 1])
        c_spread = jnp.where(own_group, c_now, 0.0)
        scores = lax.dot_general(
            c_spread.astype(BF16),
            vm[BLOCK_BPROJ][b],
            (((1,), (1,)), ((), ())),
            preferred_element_type=F32,
        )
        decays = jnp.where(live, jnp.exp(decay_rate * (step_size + later)), 0.0)
        weights = (decays * scores * steps).astype(BF16)
        inner = jnp.dot(weights, vm[BLOCK_INPUT][b], preferred_element_type=F32)
        own_score = jnp.sum(c_spread * b_now, axis=1, keepdims=True)
        carried = jnp.exp(decay_rate * (step_size + total_steps))
        c_heads = sum(
            c_spread[:, g * D_STATE : (g + 1) * D_STATE] for g in range(groups)
        )
        c_high = c_heads.astype(BF16)
        c_low = (c_heads - c_high.astype(F32)).astype(BF16)
        both = jnp.concatenate(
            [
                jnp.concatenate([c_high, c_high], axis=1),
                jnp.concatenate([c_low, jnp.zeros_like(c_low)], axis=1),
            ],
            axis=0,
        )
        doubled = lax.dot_general(
            both, state_parts, (((1,), (1,)), ((), ())), preferred_element_type=F32
        )
        readout = doubled[:heads] + doubled[heads:]
        terms = inner + (step_size * own_score) * current + carried * readout
        mixed_rows.append(jnp.sum(jnp.where(own_head, terms, 0.0), axis=0, keepdims=True))
    mixed = jnp.concatenate(mixed_rows, axis=0) * (gate_pre * lax.logistic(gate_pre))
    local[GAIN_MIX].wait()
    g_buf[me_kv] = (mixed * vm[GAIN_MIX][...]).astype(BF16)
    m_buf[me_kv] = jnp.broadcast_to(
        jnp.sum(mixed * mixed, axis=1, keepdims=True), (seqs, LANES)
    )
    copies = [
        send(g_buf.at[me_kv], g_buf.at[me_kv], g_ss.at[j - 1], g_rs.at[j - 1], {"kv": kv_peer(j)})
        for j in others
    ] + [
        send(m_buf.at[me_kv], m_buf.at[me_kv], m_ss.at[j - 1], m_rs.at[j - 1], {"kv": kv_peer(j)})
        for j in others
    ]
    local[W_OUT].wait()
    local[GAIN_MLP].wait()
    for copy in copies:
        copy.wait_recv()
    pending += copies

    unscaled = jnp.concatenate([g_buf[k].astype(F32) for k in range(kv)], axis=0).astype(BF16)
    partial_sq = jnp.concatenate([m_buf[k] for k in range(kv)], axis=0)
    share = vm[W_OUT].shape[1] // tp

    def product(q):
        start = pl.multiple_of(tp_peer(q) * share, LANES)
        return jnp.dot(unscaled, vm[W_OUT][:, pl.ds(start, share)], preferred_element_type=F32)

    copies = []
    for q in range(1, tp):
        p_send[q - 1, :, :share] = product(q)
        p_send[q - 1, :, share:] = partial_sq
        copies.append(
            send(p_send.at[q - 1], p_recv.at[q - 1], p_ss.at[q - 1], p_rs.at[q - 1], {"tp": tp_peer(q)})
        )
    summed = product(0)
    residual = stream[:, :share]
    for q in range(1, tp):
        residual = jnp.where(me_tp == q, stream[:, q * share : (q + 1) * share], residual)
    total_sq = partial_sq[:, :1]
    for q, copy in enumerate(copies):
        copy.wait_recv()
        summed = summed + p_recv[q, :, :share]
        total_sq = total_sq + p_recv[q, :, share : share + 1]
    pending += copies
    mixed_in = summed * lax.rsqrt(total_sq / (channels * tp) + EPS)
    hidden = (residual + mixed_in).astype(BF16).astype(F32)
    h_buf[me_dp] = hidden
    copies = [
        send(h_buf.at[me_dp], h_buf.at[me_dp], h_ss.at[d - 1], h_rs.at[d - 1], {"dp": dp_peer(d)})
        for d in range(1, dp)
    ]
    local[W_UP].wait()
    for copy in copies:
        copy.wait_recv()
    pending += copies

    whole_rows = jnp.concatenate([h_buf[d] for d in range(dp)], axis=0)
    lifted = (whole_rows * vm[GAIN_MLP][...]).astype(BF16)
    all_rows = rows * dp
    row_eye = lax.broadcasted_iota(jnp.int32, (all_rows, q_buf.shape[2]), 0) == (
        lax.broadcasted_iota(jnp.int32, (all_rows, q_buf.shape[2]), 1)
    )
    row_sq = jnp.sum(whole_rows * whole_rows, axis=1, keepdims=True)
    q_buf[0] = jnp.sum(jnp.where(row_eye, row_sq, 0.0), axis=0, keepdims=True)
    q_copies = [
        send(
            q_buf.at[0],
            q_buf.at[slot],
            q_ss.at[slot - 1],
            q_rs.at[slot - 1],
            {"kv": kv_peer(j), "tp": tp_peer(q)},
        )
        for slot, (j, q) in enumerate(pairs, 1)
    ]
    unit_share = vm[W_UP].shape[1] // (kv * tp)

    def raised(j):
        chip = kv_peer(j) * tp * unit_share
        columns = pl.ds(pl.multiple_of(chip, LANES), tp * unit_share)
        both = jnp.dot(lifted, vm[W_UP][:, columns], preferred_element_type=F32)
        parts = [both[:, r * unit_share : (r + 1) * unit_share] for r in range(tp)]
        picked = []
        for q in range(tp):
            piece = parts[0]
            for r in range(1, tp):
                piece = jnp.where(tp_peer(q) == r, parts[r], piece)
            picked.append(piece)
        return picked

    u_copies, r_copies = {}, {}

    def for_partner(j):
        pieces = raised(j)
        own_sum[j] = pieces[0]
        for q in range(1, tp):
            u_send[q - 1, j] = pieces[q]
            u_copies[j, q] = send(
                u_send.at[q - 1, j],
                u_recv.at[q - 1, j],
                u_ss.at[q - 1, j],
                u_rs.at[q - 1, j],
                {"tp": tp_peer(q)},
            )

    def for_chip(j):
        total = own_sum[j]
        for q in range(1, tp):
            u_copies[j, q].wait_recv()
            total = total + u_recv[q - 1, j]
        if j:
            r_send[j - 1] = total.astype(BF16)
            r_copies[j] = send(
                r_send.at[j - 1], r_recv.at[j - 1], r_ss.at[j - 1], r_rs.at[j - 1], {"kv": kv_peer(j)}
            )
        else:
            own_sum[0] = total

    for_partner(far_first[0])
    for earlier, j in zip(far_first, far_first[1:]):
        for_partner(j)
        for_chip(earlier)
    for_chip(0)
    pending += list(u_copies.values()) + list(r_copies.values()) + q_copies
    sq_row = q_buf[0]
    for slot, copy in enumerate(q_copies, 1):
        copy.wait_recv()
        sq_row = sq_row + q_buf[slot]
    sq_sum = jnp.sum(jnp.where(row_eye, sq_row, 0.0), axis=1, keepdims=True)
    inverse_mlp = lax.rsqrt(sq_sum / features + EPS)
    shares = own_sum[0]
    for j in near_first:
        r_copies[j].wait_recv()
        shares = shares + r_recv[j - 1].astype(F32)
    active = jnp.maximum(shares * inverse_mlp, 0.0)
    units[me_unit] = (active * active).astype(BF16)

    n_copies = {}
    for j in far_first:
        if j:
            n_copies[j] = send(
                units.at[me_unit], units.at[me_unit], n_ss.at[j - 1], n_rs.at[j - 1], {"kv": kv_peer(j)}
            )
    f_copies = {}

    def forward(j):
        for q in range(1, tp):
            chunk = lax.rem(me_kv + kv - j, kv) * tp + me_tp
            f_copies[j, q] = send(
                units.at[chunk], units.at[chunk], f_ss.at[q - 1, j], f_rs.at[q - 1, j], {"tp": tp_peer(q)}
            )

    def lower(j, q):
        chunk = lax.rem(me_kv + kv - j, kv) * tp + lax.rem(me_tp + tp - q, tp)
        span = pl.ds(pl.multiple_of(chunk * unit_share, LANES), unit_share)
        return jnp.dot(units[chunk], vm[W_DOWN][span, :], preferred_element_type=F32)

    forward(0)
    local[W_DOWN].wait()
    lowered = lower(0, 0)
    for q in range(1, tp):
        f_copies[0, q].wait_recv()
        lowered = lowered + lower(0, q)
    for j in near_first:
        n_copies[j].wait_recv()
        forward(j)
        lowered = lowered + lower(j, 0)
    for j in near_first:
        for q in range(1, tp):
            f_copies[j, q].wait_recv()
            lowered = lowered + lower(j, q)
    pending += list(n_copies.values()) + list(f_copies.values())

    for d in range(dp):
        l_send[d] = lowered[d * rows : (d + 1) * rows]
    copies = [
        send(l_send.at[dp_peer(d)], l_recv.at[d - 1], l_ss.at[d - 1], l_rs.at[d - 1], {"dp": dp_peer(d)})
        for d in range(1, dp)
    ]
    for copy in pending:
        copy.wait_send()
    result = h_buf[me_dp] + l_send[me_dp]
    for d, copy in enumerate(copies):
        copy.wait_recv()
        result = result + l_recv[d]
    out_ref[...] = result.astype(BF16)
    for copy in copies:
        copy.wait_send()


def fused_device(sizes, *args):
    kv, tp, dp = sizes
    named = dict(zip(NAMES, args))
    for name in (GAIN_IN, STEP_BIAS, DECAY_LOG, GAIN_MIX, GAIN_MLP):
        named[name] = named[name].reshape(1, -1)
    named[W_STEP] = named[W_STEP].T
    named[BLOCK_STEP] = named[BLOCK_STEP].transpose(0, 2, 1)
    for name in (TAIL_INPUT, TAIL_BPROJ, TAIL_CPROJ):
        named[name] = named[name].transpose(1, 0, 2)
    rows = named[INPUTS].shape[0]
    seqs = rows // kv
    pads = [
        -(-width // LANES) * LANES
        for width in [named[name].shape[1] for name in (W_GATE, W_INPUT, W_BPROJ, W_CPROJ)]
        + [named[W_STEP].shape[0]]
    ]
    wide, narrow = sum(pads[:-1]), pads[-1] + LANES
    channels = named[W_GATE].shape[1]
    share = named[W_OUT].shape[1] // tp
    all_rows = rows * dp
    unit_share = named[W_UP].shape[1] // (kv * tp)
    columns = named[W_DOWN].shape[1]
    row_lanes = -(-all_rows // LANES) * LANES
    dma = pltpu.SemaphoreType.DMA
    scratch = [pltpu.VMEM(named[name].shape, named[name].dtype) for name in COPIED] + [
        pltpu.VMEM((kv, seqs, wide), BF16),
        pltpu.VMEM((kv - 1, seqs, wide), BF16),
        pltpu.VMEM((kv, seqs, channels), BF16),
        pltpu.VMEM((tp - 1, rows, share + LANES), F32),
        pltpu.VMEM((tp - 1, rows, share + LANES), F32),
        pltpu.VMEM((dp, rows, share), F32),
        pltpu.VMEM((kv * tp, 1, row_lanes), F32),
        pltpu.VMEM((tp - 1, kv, all_rows, unit_share), F32),
        pltpu.VMEM((tp - 1, kv, all_rows, unit_share), F32),
        pltpu.VMEM((kv - 1, all_rows, unit_share), BF16),
        pltpu.VMEM((kv - 1, all_rows, unit_share), BF16),
        pltpu.VMEM((kv, all_rows, unit_share), F32),
        pltpu.VMEM((kv * tp, all_rows, unit_share), BF16),
        pltpu.VMEM((dp, rows, columns), F32),
        pltpu.VMEM((dp - 1, rows, columns), F32),
        pltpu.VMEM((kv, seqs, narrow), F32),
        pltpu.VMEM((kv - 1, seqs, narrow), F32),
        pltpu.VMEM((kv, seqs, LANES), F32),
        dma((len(COPIED),)),
        dma((kv - 1,)), dma((kv - 1,)),
        dma((kv - 1,)), dma((kv - 1,)),
        dma((tp - 1,)), dma((tp - 1,)),
        dma((dp - 1,)), dma((dp - 1,)),
        dma((kv * tp - 1,)), dma((kv * tp - 1,)),
        dma((tp - 1, kv)), dma((tp - 1, kv)),
        dma((kv - 1,)), dma((kv - 1,)),
        dma((kv - 1,)), dma((kv - 1,)),
        dma((tp - 1, kv)), dma((tp - 1, kv)),
        dma((dp - 1,)), dma((dp - 1,)),
        dma((kv - 1,)), dma((kv - 1,)),
        dma((kv - 1,)), dma((kv - 1,)),
    ]
    spaces = [
        pl.BlockSpec(memory_space=pltpu.SMEM if name == LENGTHS else pl.ANY) for name in NAMES
    ]
    return pl.pallas_call(
        functools.partial(fused, sizes),
        out_shape=jax.ShapeDtypeStruct((rows, columns), BF16),
        in_specs=spaces,
        out_specs=pl.BlockSpec(memory_space=pltpu.VMEM),
        scratch_shapes=scratch,
        compiler_params=pltpu.CompilerParams(
            collective_id=0, has_side_effects=True, vmem_limit_bytes=60 * 1024 * 1024
        ),
    )(*[named[name] for name in NAMES])


def choose(sizes, *args):
    kv, tp, _ = sizes
    named = dict(zip(NAMES, args))
    pieces = (named[W_UP].shape[1] // (kv * tp), named[W_OUT].shape[1] // tp)
    if min(sizes) > 1 and all(piece % LANES == 0 for piece in pieces):
        return fused_device(sizes, *args)
    return per_device(*args)


def solution(mesh):
    sizes = tuple(mesh.shape[axis] for axis in ("kv", "tp", "dp"))
    return jax.shard_map(
        functools.partial(choose, sizes),
        mesh=mesh,
        in_specs=(
            P(("grp", "dp"), "kv"),
            P("kv"),
            P("kv", "tp"),
            P("kv", "tp"),
            P("kv", "tp"),
            P("kv", "tp"),
            P("kv", "tp"),
            P(None, "tp"),
            P(None, "tp"),
            P(None, "tp"),
            P(("grp", "dp", "kv"), None, "tp"),
            P(("grp", "dp", "kv"), None, "tp"),
            P(("grp", "dp", "kv"), None, "tp"),
            P("tp"),
            P("tp"),
            P(("grp", "dp", "kv"), None, "tp"),
            P(("grp", "dp", "kv"), None, "tp"),
            P(("grp", "dp", "kv"), None, "tp"),
            P(("grp", "dp", "kv")),
            P(("grp", "dp", "kv"), "tp", None, None),
            P("tp"),
            P("tp", "kv"),
            P(("kv", "tp")),
            P(("kv", "tp"), "dp"),
            P("dp", ("kv", "tp")),
        ),
        out_specs=P(("grp", "dp"), ("kv", "tp")),
        check_vma=False,
    )
```

```python
import functools

import jax
import jax.numpy as jnp
from jax import lax
from jax.experimental import pallas as pl
from jax.experimental.pallas import tpu as pltpu
from jax.sharding import PartitionSpec as P

D = 4096
HEAD_DIM = 64
D_STATE = 128
TAPS = 4
SSM_WIDTH = 2048


EPS = 1e-06


def convolve(history, weights, newest):
    summed = weights[TAPS - 1] * newest
    for offset in range(TAPS - 1):
        summed = summed + weights[offset] * history[:, offset].astype(jnp.float32)
    return jax.nn.silu(summed)


def per_device(
    inputs,
    gain_in,
    w_gate,
    w_input,
    w_bproj,
    w_cproj,
    w_step,
    conv_input,
    conv_bproj,
    conv_cproj,
    tail_input,
    tail_bproj,
    tail_cproj,
    step_bias,
    decay_log,
    block_input,
    block_bproj,
    block_step,
    lengths,
    state,
    gain_mix,
    w_out,
    gain_mlp,
    w_up,
    w_down,
):
    stream = inputs.astype(jnp.float32)
    squares = jnp.sum(stream * stream, axis=1)
    scaled = (stream * gain_in).astype(jnp.bfloat16)
    matrices = (w_gate, w_input, w_bproj, w_cproj, w_step)
    pieces = [jnp.dot(scaled, weight, preferred_element_type=jnp.float32) for weight in matrices]
    projected, totals = (
        lax.psum_scatter(jnp.concatenate(pieces, axis=1), "kv", scatter_dimension=0, tiled=True),
        lax.psum_scatter(squares, "kv", scatter_dimension=0, tiled=True),
    )
    inverse = lax.rsqrt(totals / D + EPS)[:, None]
    bounds = [0]
    for weight in matrices:
        bounds.append(bounds[-1] + weight.shape[1])
    gate_pre, value_pre, b_pre, c_pre, step_pre = [
        projected[:, bounds[member] : bounds[member + 1]] * inverse for member in range(5)
    ]
    seq_count = lengths.shape[0]
    head_count = step_bias.shape[0]
    group_count = w_bproj.shape[1] // D_STATE
    block_len = block_step.shape[1]
    per_group = head_count // group_count
    current = convolve(tail_input, conv_input, value_pre)
    b_now = convolve(tail_bproj, conv_bproj, b_pre)
    c_now = convolve(tail_cproj, conv_cproj, c_pre)
    step_size = jax.nn.softplus(step_pre + step_bias)
    decay_rate = -jnp.exp(decay_log)
    positions = lax.broadcasted_iota(jnp.int32, (1, block_len), 1)
    live_rows = (positions < lengths[:, None]).astype(jnp.float32)
    masked = block_step * live_rows[:, :, None]
    later_steps = jnp.sum(masked, axis=1, keepdims=True) - jnp.cumsum(masked, axis=1)
    decays = jnp.exp(decay_rate * (step_size[:, None, :] + later_steps)) * live_rows[:, :, None]
    c_query = c_now.astype(jnp.bfloat16).reshape(seq_count, group_count, D_STATE)
    keys = block_bproj.reshape(seq_count, block_len, group_count, D_STATE)
    scores = jnp.einsum("bsgn,bgn->bsg", keys, c_query, preferred_element_type=jnp.float32)
    scores = jnp.repeat(scores, per_group, axis=2)
    weights = (decays * scores * block_step).astype(jnp.bfloat16)
    values = block_input.reshape(seq_count, block_len, head_count, HEAD_DIM)
    inner_sum = jnp.einsum("bsh,bshp->bhp", weights, values, preferred_element_type=jnp.float32)
    c_full = c_now.reshape(seq_count, group_count, D_STATE)
    b_full = b_now.reshape(seq_count, group_count, D_STATE)
    own_score = jnp.repeat(jnp.sum(c_full * b_full, axis=2), per_group, axis=1)
    own_term = (step_size * own_score)[:, :, None] * current.reshape(
        seq_count, head_count, HEAD_DIM
    )
    carried = jnp.exp(decay_rate * (step_size + jnp.sum(masked, axis=1)))
    c_heads = jnp.repeat(c_full, per_group, axis=1)
    readout = jnp.einsum("bhpn,bhn->bhp", state, c_heads, precision=lax.Precision.HIGHEST)
    mixed = (inner_sum + own_term + carried[:, :, None] * readout).reshape(
        seq_count, -1
    ) * jax.nn.silu(gate_pre)
    local_sq = jnp.sum(mixed * mixed, axis=1)
    total_sq = lax.psum(local_sq, "tp")
    normed = (mixed * lax.rsqrt(total_sq / SSM_WIDTH + EPS)[:, None] * gain_mix).astype(
        jnp.bfloat16
    )
    products = jnp.dot(
        lax.all_gather(normed, "kv", axis=0, tiled=True), w_out, preferred_element_type=jnp.float32
    )
    mixed_in = lax.psum_scatter(products, "tp", scatter_dimension=1, tiled=True)
    column_count = mixed_in.shape[1]
    residual = lax.dynamic_slice_in_dim(
        stream, lax.axis_index("tp") * column_count, column_count, 1
    )
    hidden = (residual + mixed_in).astype(jnp.bfloat16)
    lifted = (hidden.astype(jnp.float32) * gain_mlp).astype(jnp.bfloat16)
    all_lifted, all_hidden = (
        lax.all_gather(lifted, "dp", axis=0, tiled=True),
        lax.all_gather(hidden, "dp", axis=0, tiled=True),
    )
    whole_rows = all_hidden.astype(jnp.float32)
    row_sq = jnp.sum(whole_rows * whole_rows, axis=1)
    partial_value = jnp.dot(all_lifted, w_up, preferred_element_type=jnp.float32)
    sq_sum = lax.psum(row_sq, ("kv", "tp"))
    shares = lax.psum_scatter(partial_value, ("kv", "tp"), scatter_dimension=1, tiled=True)
    unit_share = jnp.square(jax.nn.relu(shares * lax.rsqrt(sq_sum / D + EPS)[:, None])).astype(
        jnp.bfloat16
    )
    hidden_units = lax.all_gather(unit_share, ("kv", "tp"), axis=1, tiled=True)
    lowered = lax.psum_scatter(
        jnp.dot(hidden_units, w_down, preferred_element_type=jnp.float32),
        "dp",
        scatter_dimension=0,
        tiled=True,
    )
    return (hidden.astype(jnp.float32) + lowered).astype(jnp.bfloat16)


MESH = pl.DeviceIdType.MESH
LANES = 128
F32 = jnp.float32
BF16 = jnp.bfloat16

(
    INPUTS,
    GAIN_IN,
    W_GATE,
    W_INPUT,
    W_BPROJ,
    W_CPROJ,
    W_STEP,
    CONV_INPUT,
    CONV_BPROJ,
    CONV_CPROJ,
    TAIL_INPUT,
    TAIL_BPROJ,
    TAIL_CPROJ,
    STEP_BIAS,
    DECAY_LOG,
    BLOCK_INPUT,
    BLOCK_BPROJ,
    BLOCK_STEP,
    LENGTHS,
    STATE,
    GAIN_MIX,
    W_OUT,
    GAIN_MLP,
    W_UP,
    W_DOWN,
) = NAMES = range(25)
EARLY = (
    INPUTS, GAIN_IN, W_STEP, W_GATE, W_INPUT, W_BPROJ, W_CPROJ,
)
MIDDLE = (
    CONV_INPUT, CONV_BPROJ, CONV_CPROJ, TAIL_INPUT, TAIL_BPROJ, TAIL_CPROJ,
    LENGTHS, STEP_BIAS, DECAY_LOG, BLOCK_STEP, BLOCK_BPROJ, BLOCK_INPUT, STATE,
    GAIN_MIX, W_OUT, GAIN_MLP,
)
LATE = (W_UP, W_DOWN)
COPIED = EARLY + MIDDLE + LATE


def send(source, target, send_sem, recv_sem, device):
    copy = pltpu.make_async_remote_copy(
        src_ref=source,
        dst_ref=target,
        send_sem=send_sem,
        recv_sem=recv_sem,
        device_id=device,
        device_id_type=MESH,
    )
    copy.start()
    return copy


def taps(history, weights, newest):
    summed = weights[TAPS - 1 :] * newest
    for offset in range(TAPS - 1):
        summed = summed + weights[offset : offset + 1] * history[offset].astype(F32)
    return summed * lax.logistic(summed)


def fused(sizes, *refs):
    kv, tp, dp = sizes
    hbm = dict(zip(NAMES, refs[: len(NAMES)]))
    out_ref = refs[len(NAMES)]
    rest = list(refs[len(NAMES) + 1 :])
    vm = dict(zip(COPIED, rest[: len(COPIED)]))
    (
        a_send, a_recv, g_buf, p_send, p_recv, h_buf, q_buf, u_send, u_recv, r_send, r_recv, own_sum,
        units, l_send, l_recv, s_send, s_recv, m_buf,
        local_sem, a_ss, a_rs, g_ss, g_rs, p_ss, p_rs, h_ss, h_rs, q_ss, q_rs, u_ss, u_rs,
        r_ss, r_rs, n_ss, n_rs, f_ss, f_rs, l_ss, l_rs, s_ss, s_rs, m_ss, m_rs,
    ) = rest[len(COPIED) :]
    me_kv, me_tp, me_dp = lax.axis_index("kv"), lax.axis_index("tp"), lax.axis_index("dp")
    me_unit = me_kv * tp + me_tp

    def kv_peer(j):
        return lax.rem(me_kv + j, kv)

    def tp_peer(q):
        return lax.rem(me_tp + q, tp)

    def dp_peer(d):
        return lax.rem(me_dp + d, dp)

    pairs = [(j, q) for j in range(kv) for q in range(tp) if j or q]
    far_first = sorted(range(kv), key=lambda j: -min(j, kv - j))
    near_first = [j for j in reversed(far_first) if j]

    barrier = pltpu.get_barrier_semaphore()
    for j, q in pairs:
        pl.semaphore_signal(
            barrier, inc=1, device_id={"kv": kv_peer(j), "tp": tp_peer(q)}, device_id_type=MESH
        )
    for d in range(1, dp):
        pl.semaphore_signal(barrier, inc=1, device_id={"dp": dp_peer(d)}, device_id_type=MESH)

    local = {
        name: pltpu.make_async_copy(hbm[name], vm[name], local_sem.at[index])
        for index, name in enumerate(COPIED)
    }
    for name in EARLY:
        local[name].start()
    pending = []

    local[INPUTS].wait()
    local[GAIN_IN].wait()
    stream = vm[INPUTS][...].astype(F32)
    rows = stream.shape[0]
    seqs = rows // kv
    scaled = (stream * vm[GAIN_IN][...]).astype(BF16)
    squares = jnp.sum(stream * stream, axis=1, keepdims=True)
    spans = {}
    at = 0
    for name in (W_GATE, W_INPUT, W_BPROJ, W_CPROJ, W_STEP):
        width = vm[name].shape[name != W_STEP]
        spans[name] = (at, at + width) if name != W_STEP else (0, width)
        local[name].wait()
        if name == W_GATE:
            for other in MIDDLE:
                local[other].start()
        if name == W_STEP:
            at = 0
        piece = lax.dot_general(
            scaled,
            vm[name][...],
            (((1,), (int(name == W_STEP),)), ((), ())),
            preferred_element_type=F32,
        )
        for k in range(kv):
            if name == W_STEP:
                s_send[k, :, :width] = piece[k * seqs : (k + 1) * seqs]
            else:
                a_send[k, :, at : at + width] = piece[k * seqs : (k + 1) * seqs].astype(BF16)
        at += -(-width // LANES) * LANES
    wide_squares = jnp.broadcast_to(squares, (rows, LANES))
    for k in range(kv):
        s_send[k, :, at : at + LANES] = wide_squares[k * seqs : (k + 1) * seqs]
    for name in LATE:
        local[name].start()
    pl.semaphore_wait(barrier, len(pairs) + dp - 1)
    others = [j for j in far_first if j]
    copies = [
        send(a_send.at[kv_peer(j)], a_recv.at[j - 1], a_ss.at[j - 1], a_rs.at[j - 1], {"kv": kv_peer(j)})
        for j in others
    ]
    s_copies = [
        send(s_send.at[kv_peer(j)], s_recv.at[j - 1], s_ss.at[j - 1], s_rs.at[j - 1], {"kv": kv_peer(j)})
        for j in others
    ]

    for name in MIDDLE[:-3]:
        local[name].wait()
    heads = vm[STEP_BIAS].shape[1]
    groups = vm[W_BPROJ].shape[1] // D_STATE
    per_group = heads // groups
    channels = heads * HEAD_DIM
    block = vm[BLOCK_STEP].shape[2]
    head_eye = lax.broadcasted_iota(jnp.int32, (heads, heads), 0) == lax.broadcasted_iota(
        jnp.int32, (heads, heads), 1
    )

    def column(row):
        return jnp.sum(jnp.where(head_eye, row, 0.0), axis=1, keepdims=True)

    later_than = (
        lax.broadcasted_iota(jnp.int32, (block, block), 0)
        > lax.broadcasted_iota(jnp.int32, (block, block), 1)
    ).astype(F32)
    positions = lax.broadcasted_iota(jnp.int32, (heads, block), 1)
    decay_rate = column(-jnp.exp(vm[DECAY_LOG][...]))
    prepared = []
    for b in range(seqs):
        live = positions < vm[LENGTHS][b]
        steps = vm[BLOCK_STEP][b]
        masked = jnp.where(live, steps, 0.0)
        later = jnp.dot(
            masked, later_than, precision=lax.Precision.HIGHEST, preferred_element_type=F32
        )
        state = vm[STATE][b].reshape(channels, D_STATE)
        high = state.astype(BF16)
        state_parts = jnp.concatenate([high, (state - high.astype(F32)).astype(BF16)], axis=1)
        prepared.append((live, steps, later, jnp.sum(masked, axis=1, keepdims=True), state_parts))
    own_head = lax.broadcasted_iota(jnp.int32, (heads, channels), 0) == (
        lax.broadcasted_iota(jnp.int32, (heads, channels), 1) // HEAD_DIM
    )
    own_group = (lax.broadcasted_iota(jnp.int32, (heads, groups * D_STATE), 0) // per_group) == (
        lax.broadcasted_iota(jnp.int32, (heads, groups * D_STATE), 1) // D_STATE
    )

    projected = a_send[me_kv].astype(F32)
    stepped = s_send[me_kv]
    for copy, s_copy, j in zip(copies, s_copies, others):
        copy.wait_recv()
        s_copy.wait_recv()
        projected = projected + a_recv[j - 1].astype(F32)
        stepped = stepped + s_recv[j - 1]
    pending += copies + s_copies
    features = vm[INPUTS].shape[1] * kv
    inverse = lax.rsqrt(stepped[:, at : at + 1] / features + EPS)

    def part(name):
        source = stepped if name == W_STEP else projected
        return source[:, spans[name][0] : spans[name][1]] * inverse

    gate_pre, value_pre, b_pre, c_pre, step_pre = [
        part(name) for name in (W_GATE, W_INPUT, W_BPROJ, W_CPROJ, W_STEP)
    ]
    biased = step_pre + vm[STEP_BIAS][...]
    softened = jnp.maximum(biased, 0.0) + jnp.log1p(jnp.exp(-jnp.abs(biased)))
    mixed_rows = []
    all_current = taps(vm[TAIL_INPUT], vm[CONV_INPUT][...], value_pre)
    all_b = taps(vm[TAIL_BPROJ], vm[CONV_BPROJ][...], b_pre)
    all_c = taps(vm[TAIL_CPROJ], vm[CONV_CPROJ][...], c_pre)
    for b in range(seqs):
        live, steps, later, total_steps, state_parts = prepared[b]
        current, b_now, c_now = all_current[b : b + 1], all_b[b : b + 1], all_c[b : b + 1]
        step_size = column(softened[b : b + 1])
        c_spread = jnp.where(own_group, c_now, 0.0)
        scores = lax.dot_general(
            c_spread.astype(BF16),
            vm[BLOCK_BPROJ][b],
            (((1,), (1,)), ((), ())),
            preferred_element_type=F32,
        )
        decays = jnp.where(live, jnp.exp(decay_rate * (step_size + later)), 0.0)
        weights = (decays * scores * steps).astype(BF16)
        inner = jnp.dot(weights, vm[BLOCK_INPUT][b], preferred_element_type=F32)
        own_score = jnp.sum(c_spread * b_now, axis=1, keepdims=True)
        carried = jnp.exp(decay_rate * (step_size + total_steps))
        c_heads = sum(
            c_spread[:, g * D_STATE : (g + 1) * D_STATE] for g in range(groups)
        )
        c_high = c_heads.astype(BF16)
        c_low = (c_heads - c_high.astype(F32)).astype(BF16)
        both = jnp.concatenate(
            [
                jnp.concatenate([c_high, c_high], axis=1),
                jnp.concatenate([c_low, jnp.zeros_like(c_low)], axis=1),
            ],
            axis=0,
        )
        doubled = lax.dot_general(
            both, state_parts, (((1,), (1,)), ((), ())), preferred_element_type=F32
        )
        readout = doubled[:heads] + doubled[heads:]
        terms = inner + (step_size * own_score) * current + carried * readout
        mixed_rows.append(jnp.sum(jnp.where(own_head, terms, 0.0), axis=0, keepdims=True))
    mixed = jnp.concatenate(mixed_rows, axis=0) * (gate_pre * lax.logistic(gate_pre))
    local[GAIN_MIX].wait()
    g_buf[me_kv] = (mixed * vm[GAIN_MIX][...]).astype(BF16)
    m_buf[me_kv] = jnp.broadcast_to(
        jnp.sum(mixed * mixed, axis=1, keepdims=True), (seqs, LANES)
    )
    copies = [
        send(g_buf.at[me_kv], g_buf.at[me_kv], g_ss.at[j - 1], g_rs.at[j - 1], {"kv": kv_peer(j)})
        for j in others
    ] + [
        send(m_buf.at[me_kv], m_buf.at[me_kv], m_ss.at[j - 1], m_rs.at[j - 1], {"kv": kv_peer(j)})
        for j in others
    ]
    local[W_OUT].wait()
    local[GAIN_MLP].wait()
    for copy in copies:
        copy.wait_recv()
    pending += copies

    unscaled = jnp.concatenate([g_buf[k].astype(F32) for k in range(kv)], axis=0).astype(BF16)
    partial_sq = jnp.concatenate([m_buf[k] for k in range(kv)], axis=0)
    share = vm[W_OUT].shape[1] // tp

    def product(q):
        start = pl.multiple_of(tp_peer(q) * share, LANES)
        return jnp.dot(unscaled, vm[W_OUT][:, pl.ds(start, share)], preferred_element_type=F32)

    copies = []
    for q in range(1, tp):
        p_send[q - 1, :, :share] = product(q)
        p_send[q - 1, :, share:] = partial_sq
        copies.append(
            send(p_send.at[q - 1], p_recv.at[q - 1], p_ss.at[q - 1], p_rs.at[q - 1], {"tp": tp_peer(q)})
        )
    summed = product(0)
    residual = stream[:, :share]
    for q in range(1, tp):
        residual = jnp.where(me_tp == q, stream[:, q * share : (q + 1) * share], residual)
    total_sq = partial_sq[:, :1]
    for q, copy in enumerate(copies):
        copy.wait_recv()
        summed = summed + p_recv[q, :, :share]
        total_sq = total_sq + p_recv[q, :, share : share + 1]
    pending += copies
    mixed_in = summed * lax.rsqrt(total_sq / (channels * tp) + EPS)
    hidden = (residual + mixed_in).astype(BF16).astype(F32)
    h_buf[me_dp] = hidden
    copies = [
        send(h_buf.at[me_dp], h_buf.at[me_dp], h_ss.at[d - 1], h_rs.at[d - 1], {"dp": dp_peer(d)})
        for d in range(1, dp)
    ]
    local[W_UP].wait()
    for copy in copies:
        copy.wait_recv()
    pending += copies

    whole_rows = jnp.concatenate([h_buf[d] for d in range(dp)], axis=0)
    lifted = (whole_rows * vm[GAIN_MLP][...]).astype(BF16)
    all_rows = rows * dp
    row_eye = lax.broadcasted_iota(jnp.int32, (all_rows, q_buf.shape[2]), 0) == (
        lax.broadcasted_iota(jnp.int32, (all_rows, q_buf.shape[2]), 1)
    )
    row_sq = jnp.sum(whole_rows * whole_rows, axis=1, keepdims=True)
    q_buf[0] = jnp.sum(jnp.where(row_eye, row_sq, 0.0), axis=0, keepdims=True)
    q_copies = [
        send(
            q_buf.at[0],
            q_buf.at[slot],
            q_ss.at[slot - 1],
            q_rs.at[slot - 1],
            {"kv": kv_peer(j), "tp": tp_peer(q)},
        )
        for slot, (j, q) in enumerate(pairs, 1)
    ]
    unit_share = vm[W_UP].shape[1] // (kv * tp)

    def raised(j):
        chip = kv_peer(j) * tp * unit_share
        columns = pl.ds(pl.multiple_of(chip, LANES), tp * unit_share)
        both = jnp.dot(lifted, vm[W_UP][:, columns], preferred_element_type=F32)
        parts = [both[:, r * unit_share : (r + 1) * unit_share] for r in range(tp)]
        picked = []
        for q in range(tp):
            piece = parts[0]
            for r in range(1, tp):
                piece = jnp.where(tp_peer(q) == r, parts[r], piece)
            picked.append(piece)
        return picked

    u_copies, r_copies = {}, {}

    def for_partner(j):
        pieces = raised(j)
        own_sum[j] = pieces[0]
        for q in range(1, tp):
            u_send[q - 1, j] = pieces[q]
            u_copies[j, q] = send(
                u_send.at[q - 1, j],
                u_recv.at[q - 1, j],
                u_ss.at[q - 1, j],
                u_rs.at[q - 1, j],
                {"tp": tp_peer(q)},
            )

    def for_chip(j):
        total = own_sum[j]
        for q in range(1, tp):
            u_copies[j, q].wait_recv()
            total = total + u_recv[q - 1, j]
        if j:
            r_send[j - 1] = total.astype(BF16)
            r_copies[j] = send(
                r_send.at[j - 1], r_recv.at[j - 1], r_ss.at[j - 1], r_rs.at[j - 1], {"kv": kv_peer(j)}
            )
        else:
            own_sum[0] = total

    for_partner(far_first[0])
    for earlier, j in zip(far_first, far_first[1:]):
        for_partner(j)
        for_chip(earlier)
    for_chip(0)
    pending += list(u_copies.values()) + list(r_copies.values()) + q_copies
    sq_row = q_buf[0]
    for slot, copy in enumerate(q_copies, 1):
        copy.wait_recv()
        sq_row = sq_row + q_buf[slot]
    sq_sum = jnp.sum(jnp.where(row_eye, sq_row, 0.0), axis=1, keepdims=True)
    inverse_mlp = lax.rsqrt(sq_sum / features + EPS)
    shares = own_sum[0]
    for j in near_first:
        r_copies[j].wait_recv()
        shares = shares + r_recv[j - 1].astype(F32)
    active = jnp.maximum(shares * inverse_mlp, 0.0)
    units[me_unit] = (active * active).astype(BF16)

    n_copies = {}
    for j in far_first:
        if j:
            n_copies[j] = send(
                units.at[me_unit], units.at[me_unit], n_ss.at[j - 1], n_rs.at[j - 1], {"kv": kv_peer(j)}
            )
    f_copies = {}

    def forward(j):
        for q in range(1, tp):
            chunk = lax.rem(me_kv + kv - j, kv) * tp + me_tp
            f_copies[j, q] = send(
                units.at[chunk], units.at[chunk], f_ss.at[q - 1, j], f_rs.at[q - 1, j], {"tp": tp_peer(q)}
            )

    def lower(j, q):
        chunk = lax.rem(me_kv + kv - j, kv) * tp + lax.rem(me_tp + tp - q, tp)
        span = pl.ds(pl.multiple_of(chunk * unit_share, LANES), unit_share)
        return jnp.dot(units[chunk], vm[W_DOWN][span, :], preferred_element_type=F32)

    forward(0)
    local[W_DOWN].wait()
    lowered = lower(0, 0)
    for q in range(1, tp):
        f_copies[0, q].wait_recv()
        lowered = lowered + lower(0, q)
    for j in near_first:
        n_copies[j].wait_recv()
        forward(j)
        lowered = lowered + lower(j, 0)
    for j in near_first:
        for q in range(1, tp):
            f_copies[j, q].wait_recv()
            lowered = lowered + lower(j, q)
    pending += list(n_copies.values()) + list(f_copies.values())

    for d in range(dp):
        l_send[d] = lowered[d * rows : (d + 1) * rows]
    copies = [
        send(l_send.at[dp_peer(d)], l_recv.at[d - 1], l_ss.at[d - 1], l_rs.at[d - 1], {"dp": dp_peer(d)})
        for d in range(1, dp)
    ]
    for copy in pending:
        copy.wait_send()
    result = h_buf[me_dp] + l_send[me_dp]
    for d, copy in enumerate(copies):
        copy.wait_recv()
        result = result + l_recv[d]
    out_ref[...] = result.astype(BF16)
    for copy in copies:
        copy.wait_send()


def fused_device(sizes, *args):
    kv, tp, dp = sizes
    named = dict(zip(NAMES, args))
    for name in (GAIN_IN, STEP_BIAS, DECAY_LOG, GAIN_MIX, GAIN_MLP):
        named[name] = named[name].reshape(1, -1)
    named[W_STEP] = named[W_STEP].T
    named[BLOCK_STEP] = named[BLOCK_STEP].transpose(0, 2, 1)
    for name in (TAIL_INPUT, TAIL_BPROJ, TAIL_CPROJ):
        named[name] = named[name].transpose(1, 0, 2)
    rows = named[INPUTS].shape[0]
    seqs = rows // kv
    pads = [
        -(-width // LANES) * LANES
        for width in [named[name].shape[1] for name in (W_GATE, W_INPUT, W_BPROJ, W_CPROJ)]
        + [named[W_STEP].shape[0]]
    ]
    wide, narrow = sum(pads[:-1]), pads[-1] + LANES
    channels = named[W_GATE].shape[1]
    share = named[W_OUT].shape[1] // tp
    all_rows = rows * dp
    unit_share = named[W_UP].shape[1] // (kv * tp)
    columns = named[W_DOWN].shape[1]
    row_lanes = -(-all_rows // LANES) * LANES
    dma = pltpu.SemaphoreType.DMA
    scratch = [
        (pltpu.SMEM if name == LENGTHS else pltpu.VMEM)(named[name].shape, named[name].dtype)
        for name in COPIED
    ] + [
        pltpu.VMEM((kv, seqs, wide), BF16),
        pltpu.VMEM((kv - 1, seqs, wide), BF16),
        pltpu.VMEM((kv, seqs, channels), BF16),
        pltpu.VMEM((tp - 1, rows, share + LANES), F32),
        pltpu.VMEM((tp - 1, rows, share + LANES), F32),
        pltpu.VMEM((dp, rows, share), F32),
        pltpu.VMEM((kv * tp, 1, row_lanes), F32),
        pltpu.VMEM((tp - 1, kv, all_rows, unit_share), F32),
        pltpu.VMEM((tp - 1, kv, all_rows, unit_share), F32),
        pltpu.VMEM((kv - 1, all_rows, unit_share), BF16),
        pltpu.VMEM((kv - 1, all_rows, unit_share), BF16),
        pltpu.VMEM((kv, all_rows, unit_share), F32),
        pltpu.VMEM((kv * tp, all_rows, unit_share), BF16),
        pltpu.VMEM((dp, rows, columns), F32),
        pltpu.VMEM((dp - 1, rows, columns), F32),
        pltpu.VMEM((kv, seqs, narrow), F32),
        pltpu.VMEM((kv - 1, seqs, narrow), F32),
        pltpu.VMEM((kv, seqs, LANES), F32),
        dma((len(COPIED),)),
        dma((kv - 1,)), dma((kv - 1,)),
        dma((kv - 1,)), dma((kv - 1,)),
        dma((tp - 1,)), dma((tp - 1,)),
        dma((dp - 1,)), dma((dp - 1,)),
        dma((kv * tp - 1,)), dma((kv * tp - 1,)),
        dma((tp - 1, kv)), dma((tp - 1, kv)),
        dma((kv - 1,)), dma((kv - 1,)),
        dma((kv - 1,)), dma((kv - 1,)),
        dma((tp - 1, kv)), dma((tp - 1, kv)),
        dma((dp - 1,)), dma((dp - 1,)),
        dma((kv - 1,)), dma((kv - 1,)),
        dma((kv - 1,)), dma((kv - 1,)),
    ]
    spaces = [pl.BlockSpec(memory_space=pl.ANY) for name in NAMES]
    return pl.pallas_call(
        functools.partial(fused, sizes),
        out_shape=jax.ShapeDtypeStruct((rows, columns), BF16),
        in_specs=spaces,
        out_specs=pl.BlockSpec(memory_space=pltpu.VMEM),
        scratch_shapes=scratch,
        compiler_params=pltpu.CompilerParams(
            collective_id=0, has_side_effects=True, vmem_limit_bytes=60 * 1024 * 1024
        ),
    )(*[named[name] for name in NAMES])


def choose(sizes, *args):
    kv, tp, _ = sizes
    named = dict(zip(NAMES, args))
    pieces = (named[W_UP].shape[1] // (kv * tp), named[W_OUT].shape[1] // tp)
    if min(sizes) > 1 and all(piece % LANES == 0 for piece in pieces):
        return fused_device(sizes, *args)
    return per_device(*args)


def solution(mesh):
    sizes = tuple(mesh.shape[axis] for axis in ("kv", "tp", "dp"))
    return jax.shard_map(
        functools.partial(choose, sizes),
        mesh=mesh,
        in_specs=(
            P(("grp", "dp"), "kv"),
            P("kv"),
            P("kv", "tp"),
            P("kv", "tp"),
            P("kv", "tp"),
            P("kv", "tp"),
            P("kv", "tp"),
            P(None, "tp"),
            P(None, "tp"),
            P(None, "tp"),
            P(("grp", "dp", "kv"), None, "tp"),
            P(("grp", "dp", "kv"), None, "tp"),
            P(("grp", "dp", "kv"), None, "tp"),
            P("tp"),
            P("tp"),
            P(("grp", "dp", "kv"), None, "tp"),
            P(("grp", "dp", "kv"), None, "tp"),
            P(("grp", "dp", "kv"), None, "tp"),
            P(("grp", "dp", "kv")),
            P(("grp", "dp", "kv"), "tp", None, None),
            P("tp"),
            P("tp", "kv"),
            P(("kv", "tp")),
            P(("kv", "tp"), "dp"),
            P("dp", ("kv", "tp")),
        ),
        out_specs=P(("grp", "dp"), ("kv", "tp")),
        check_vma=False,
    )
```
